256 devices in a mesh: grp: 2 (over y), sp: 16 (over z), fs: 4 (over x), tp: 2 (over core).
Axes of the slice: x: 4, y: 2, z: 16, core: 2. Of those that a mesh axis runs over, the one named last changes fastest.
The devices are a block of a 4x16x16 slice.
Arguments:
- tokens: bfloat16 [8, 8192, 2048], P(('grp', 'fs'), ('sp', 'tp')), parts along dimension 0, may hold values from -6 to 6
- norm_gain: float32 [2048], replicated, may hold values from 0.1 to 1.9
- w_bgate: bfloat16 [2048, 2048], P(('sp', 'fs'), 'tp'), may hold values from -0.125 to 0.125
- w_cgate: bfloat16 [2048, 2048], P(('sp', 'fs'), 'tp'), may hold values from -0.125 to 0.125
- w_conv_in: bfloat16 [2048, 2048], P(('sp', 'fs'), 'tp'), may hold values from -0.125 to 0.125
- conv_taps: bfloat16 [3, 2048], P(None, 'tp'), may hold values from -3.5 to 3.5
- w_query: bfloat16 [2048, 2048], P(('sp', 'fs'), 'tp'), may hold values from -0.13258252 to 0.13258252
- w_key: bfloat16 [2048, 256], P(('sp', 'fs'), 'tp'), may hold values from -4.02167 to 4.02167
- w_value: bfloat16 [2048, 256], P(('sp', 'fs'), 'tp'), may hold values from -0.125 to 0.125
- sink_logits: float32 [32], P('tp'), may hold values from 1 to 6
- conv_out_weight: bfloat16 [2048, 2048], P('tp', ('sp', 'fs')), may hold values from -0.125 to 0.125
- attn_out_weight: bfloat16 [2048, 2048], P('tp', ('sp', 'fs')), may hold values from -0.75 to 0.75
Outputs:
- mixed: bfloat16 [8, 8192, 2048], P(('grp', 'fs'), ('sp', 'tp')), parts along dimension 0
The draws below stay inside these ranges and needn't reach their ends.
There are 2 independent parts, one for each index of `grp`. The reference program is written for one: setup_inputs(seed, part) draws one part's arguments, and reference() takes and returns one part's arrays. A program takes and returns all parts, laid end to end along the dimension named above; an argument that names none is the same for every part. Nothing has to cross between parts.
All inputs are finite; a program needn't handle non-finite values.
Results may differ from the reference program's by a relative error of at most 0.014.
The reference program's roundings to bfloat16 on the way count: a program that leaves them out, or rounds other values in their place, can miss the bound.
Values may be sent and summed in bfloat16 or wider, within the bound.
A program may use at most 128 MiB of HBM per device.

```python
import jax
import jax.numpy as jnp
from jax import lax

D = 2048
CONV = 2048
HEADS = 32
KV_HEADS = 4
HEAD = 64
WINDOW = 128
TAPS = 3
ATTN_Q = 2048
ATTN_KV = 256
SEQS = 4
LENGTH = 8192
N_TP = 2


def query_matrix(key):
    raw = jax.random.normal(jax.random.fold_in(key, 31), (D, ATTN_Q), jnp.float32)
    return jnp.clip(raw, -6.0, 6.0) / jnp.sqrt(jnp.float32(D))


def draw_w_query(key, part):
    return query_matrix(key).astype(jnp.bfloat16)


def draw_w_key(key, part):
    raw = jax.random.normal(jax.random.fold_in(key, 32), (D, ATTN_KV), jnp.float32)
    noise = jnp.clip(raw, -6.0, 6.0) / jnp.sqrt(jnp.float32(D))
    return noise.astype(jnp.bfloat16)


def draw_tokens(key, part):
    base = jnp.clip(jax.random.normal(jax.random.fold_in(key, 41), (SEQS, LENGTH, D), jnp.float32), -6.0, 6.0)
    return base.astype(jnp.bfloat16)


def steps_of(rng, shape, shards, smallest, high):
    gain = 1.0
    for dim, parts in shards:
        draws = jax.random.uniform(jax.random.fold_in(jax.random.fold_in(rng, 6), dim), (parts,), jnp.float32, smallest / len(shards), high / len(shards))
        gain = gain * jnp.repeat(jnp.exp(draws), shape[dim] // parts).reshape((-1,) + (1,) * (len(shape) - 1 - dim))
    return gain


def normal_values(own_key, shape, spread, bound, pieces=(), kind=jnp.bfloat16):
    array = jax.random.normal(own_key, shape, jnp.float32) * spread
    if len(pieces) > 0:
        array = steps_of(own_key, shape, pieces, -0.22, 0.18) * array
    return jnp.clip(array, min=-bound, max=bound).astype(kind)


def setup_inputs(seed: int = 0, part: int = 0) -> dict:
    key_list = jax.random.split(jax.random.key(seed), 13)
    own_keys = jax.random.split(jax.random.fold_in(key_list[12], part), 13)
    return {
        "tokens": draw_tokens(jax.random.fold_in(jax.random.fold_in(key_list[12], part), 71), part),
        "norm_gain": jnp.clip(1.0 + 0.18 * jax.random.normal(key_list[1], (D,), jnp.float32), 0.1, 1.9),
        "w_bgate": normal_values(key_list[2], (D, CONV), D ** -0.5, 0.125, ((0, 64), (1, 2))),
        "w_cgate": normal_values(key_list[3], (D, CONV), D ** -0.5, 0.125, ((0, 64), (1, 2))),
        "w_conv_in": normal_values(key_list[4], (D, CONV), D ** -0.5, 0.125, ((0, 64), (1, 2))),
        "conv_taps": normal_values(key_list[5], (TAPS, CONV), TAPS ** -0.5, 3.5, ((1, 2),)),
        "w_query": draw_w_query(jax.random.fold_in(key_list[12], 71), part),
        "w_key": draw_w_key(jax.random.fold_in(key_list[12], 71), part),
        "w_value": normal_values(key_list[8], (D, ATTN_KV), D ** -0.5, 0.125, ((0, 64), (1, 2))),
        "sink_logits": jnp.clip(1.0 + 5.0 * jax.random.uniform(key_list[9], (HEADS,), jnp.float32) ** steps_of(key_list[9], (HEADS,), ((0, 2),), -0.2, 0.2), 1.0, 6.0),
        "conv_out_weight": normal_values(key_list[10], (CONV, D), CONV ** -0.5, 0.125, ((0, 2), (1, 64))),
        "attn_out_weight": normal_values(key_list[11], (ATTN_Q, D), (ATTN_Q // 32) ** -0.5, 0.75, ((0, 2), (1, 64))),
    }


epsilon = 1e-06

def window_attention(queries, key_rows, value_rows, sink_logits):
    length = queries.shape[0]
    blocks = length // WINDOW
    groups = HEADS // KV_HEADS
    query_blocks = queries.astype(jnp.float32).reshape(blocks, WINDOW, KV_HEADS, groups, HEAD)
    zero_rows = jnp.zeros((WINDOW, ATTN_KV), jnp.float32)
    key_all = jnp.concatenate([zero_rows, key_rows.astype(jnp.float32)], 0)
    value_all = jnp.concatenate([zero_rows, value_rows.astype(jnp.float32)], 0)
    key_band = jnp.concatenate([key_all[:length].reshape(blocks, WINDOW, KV_HEADS, HEAD), key_all[WINDOW:].reshape(blocks, WINDOW, KV_HEADS, HEAD)], 1)
    value_band = jnp.concatenate([value_all[:length].reshape(blocks, WINDOW, KV_HEADS, HEAD), value_all[WINDOW:].reshape(blocks, WINDOW, KV_HEADS, HEAD)], 1)
    scores = jnp.einsum('nqhgd,nkhd->nhgqk', query_blocks, key_band) / jnp.sqrt(jnp.float32(HEAD))
    block_ids = jnp.arange(blocks)[:, None, None]
    query_pos = block_ids * WINDOW + jnp.arange(WINDOW)[None, :, None]
    key_pos = (block_ids - 1) * WINDOW + jnp.arange(2 * WINDOW)[None, None, :]
    allowed = (key_pos >= 0) & (key_pos <= query_pos) & (query_pos - key_pos < WINDOW)
    scores = jnp.where(allowed[:, None, None], scores, -jnp.inf)
    sink_grid = sink_logits.astype(jnp.float32).reshape(1, KV_HEADS, groups, 1, 1)
    peak_score = jnp.maximum(lax.optimization_barrier(jnp.max(scores, axis=-1, keepdims=True)), sink_grid)
    weights = jnp.exp(scores - peak_score)
    denominator = lax.optimization_barrier(jnp.sum(weights, axis=-1, keepdims=True)) + jnp.exp(sink_grid - peak_score)
    probabilities = (weights / denominator).astype(jnp.bfloat16)
    attended = jnp.einsum('nhgqk,nkhd->nqhgd', probabilities.astype(jnp.float32), value_band)
    return attended.astype(jnp.bfloat16).reshape(length, ATTN_Q)

def one_sequence(tokens, norm_gain, w_bgate, w_cgate, w_conv_in, conv_taps, w_query, w_key, w_value, sink_logits, conv_out_weight, attn_out_weight):
    widened = tokens.astype(jnp.float32)
    normed = (widened * lax.rsqrt(lax.optimization_barrier(jnp.mean(widened * widened, axis=-1, keepdims=True)) + epsilon) * norm_gain).astype(jnp.bfloat16)

    def project(weight):
        return jnp.dot(normed, weight, preferred_element_type=jnp.float32).astype(jnp.bfloat16)
    out_gate = project(w_bgate)
    in_gate = project(w_cgate)
    conv_input = project(w_conv_in)
    queries = project(w_query)
    key_rows = project(w_key)
    value_rows = project(w_value)
    length = tokens.shape[0]
    gated = (in_gate.astype(jnp.float32) * conv_input.astype(jnp.float32)).astype(jnp.bfloat16)
    padded = jnp.concatenate([jnp.zeros((TAPS - 1, CONV), jnp.bfloat16), gated], 0)
    taps_wide = conv_taps.astype(jnp.float32)
    convolved = padded[0:length].astype(jnp.float32) * taps_wide[0]
    for which in range(1, TAPS):
        convolved = convolved + padded[which:which + length].astype(jnp.float32) * taps_wide[which]
    conv_branch = (out_gate.astype(jnp.float32) * convolved).astype(jnp.bfloat16)
    attended = window_attention(queries, key_rows, value_rows, sink_logits)
    conv_parts = conv_branch.reshape(length, N_TP, CONV // N_TP)
    attn_parts = attended.reshape(length, N_TP, ATTN_Q // N_TP)
    conv_weight_parts = conv_out_weight.reshape(N_TP, CONV // N_TP, D)
    attn_weight_parts = attn_out_weight.reshape(N_TP, ATTN_Q // N_TP, D)
    running = jnp.zeros((length, D), jnp.float32)
    for member in range(N_TP):
        partial_value = jnp.dot(conv_parts[:, member], conv_weight_parts[member], preferred_element_type=jnp.float32)
        partial_value = partial_value + jnp.dot(attn_parts[:, member], attn_weight_parts[member], preferred_element_type=jnp.float32)
        rounded = lax.optimization_barrier(partial_value.astype(jnp.bfloat16))
        running = running + rounded.astype(jnp.float32)
    return running.astype(jnp.bfloat16)

def reference(tokens, norm_gain, w_bgate, w_cgate, w_conv_in, conv_taps, w_query, w_key, w_value, sink_logits, conv_out_weight, attn_out_weight):
    results = []
    for sequence in range(SEQS):
        results.append(one_sequence(tokens[sequence], norm_gain, w_bgate, w_cgate, w_conv_in, conv_taps, w_query, w_key, w_value, sink_logits, conv_out_weight, attn_out_weight))
    return jnp.stack(results, 0)
```

```python
import functools

import jax
import jax.numpy as jnp
from jax import lax
from jax.experimental import pallas as pl
from jax.experimental.pallas import tpu as pltpu
from jax.sharding import PartitionSpec as P

HEAD = 64
WINDOW = 128
TAPS = 3
EPSILON = 1e-06
MESH = pl.DeviceIdType.MESH
F32 = jnp.float32
BF16 = jnp.bfloat16
TILE = 256


def rows_dot(a, b):
    return lax.dot_general(a, b, (((1,), (1,)), ((), ())), preferred_element_type=F32)


def layer_kernel(
    ns,
    nf,
    xn,
    w_query,
    w_conv_in,
    w_cgate,
    w_bgate,
    kv_pack,
    out_pack,
    aux_in,
    out,
    x_all,
    w_in,
    w_out,
    proj,
    kv_rows,
    gated,
    acts,
    aux,
    send_far,
    recv_far,
    send_near,
    recv_near,
    own_sum,
    first_send,
    first_recv,
    z_send,
    z_recv,
    p_send,
    p_recv,
    x_send,
    x_recv,
    aux_send,
    aux_recv,
    halo_send,
    halo_recv,
    far_send,
    far_recv,
    near_send,
    near_recv,
):
    s = lax.axis_index("sp")
    f = lax.axis_index("fs")
    t = lax.axis_index("tp")
    s_next, s_prev = lax.rem(s + 1, ns), lax.rem(s + ns - 1, ns)
    f_next, f_prev = lax.rem(f + 1, nf), lax.rem(f + nf - 1, nf)
    f_far = lax.rem(f + 2, nf)
    other = 1 - t
    rows, width = xn.shape
    rb = w_query.shape[0]
    quarter = w_query.shape[1] // 2
    kvw = kv_pack.shape[2]
    half = rows // 2
    blocks = rows // WINDOW

    def remote(src, dst, send_sem, recv_sem, **where):
        return pltpu.make_async_remote_copy(
            src_ref=src,
            dst_ref=dst,
            send_sem=send_sem,
            recv_sem=recv_sem,
            device_id=where,
            device_id_type=MESH,
        )

    barrier = pltpu.get_barrier_semaphore()
    for df in range(nf):
        for dt in range(2):
            if df == 0 and dt == 0:
                continue
            pl.semaphore_signal(
                barrier,
                inc=1,
                device_id={"fs": lax.rem(f + df, nf), "tp": lax.rem(t + dt, 2)},
                device_id_type=MESH,
            )
    for neighbour in (s_next, s_prev):
        for dt in range(2):
            pl.semaphore_signal(
                barrier,
                inc=1,
                device_id={"sp": neighbour, "tp": lax.rem(t + dt, 2)},
                device_id_type=MESH,
            )
    pl.semaphore_wait(barrier, 2 * nf - 1 + 4)

    weights = (w_in, w_out)
    mine = f // 2
    for j in range(2):
        to_f = 2 * t + j
        sources = [w.at[:, pl.ds(j * quarter, quarter)] for w in (w_query, w_conv_in, w_cgate, w_bgate)]
        sources.append(kv_pack.at[j])
        spans = [pl.ds(n * quarter, quarter) for n in range(4)] + [pl.ds(4 * quarter, kvw)]
        slot = pl.ds(lax.rem(f, 2) * rb, rb)
        here = jnp.logical_and(to_f == f, mine == t)

        @pl.when(jnp.logical_not(here))
        def _():
            for src, span in zip(sources, spans):
                remote(
                    src,
                    w_in.at[s, mine, slot, span],
                    first_send.at[0, j],
                    first_recv.at[0, lax.rem(f, 2)],
                    fs=to_f,
                    tp=mine,
                ).start()
            remote(
                out_pack.at[j],
                w_out.at[s, mine, slot],
                first_send.at[1, j],
                first_recv.at[1, lax.rem(f, 2)],
                fs=to_f,
                tp=mine,
            ).start()

        @pl.when(here)
        def _():
            for src, span in zip(sources, spans):
                w_in[s, mine, slot, span] = src[...]
            w_out[s, mine, slot] = out_pack[j]

    remote(aux_in, aux.at[t], aux_send, aux_recv, tp=other).start()

    halves = (pl.ds(0, half), pl.ds(half, half))
    for which in (0, 1):
        remote(xn.at[halves[which]], x_all.at[f, halves[which]], x_send.at[0], x_recv.at[0, which], fs=f_next).start()
        remote(xn.at[halves[1 - which]], x_all.at[f, halves[1 - which]], x_send.at[1], x_recv.at[1, 1 - which], fs=f_prev).start()
    x_all[f] = xn[...]
    aux[t] = aux_in[...]

    def wait_first(k):
        for i in range(2):
            local = jnp.logical_and(t == f // 2, f == 2 * t + i)

            @pl.when(jnp.logical_not(local))
            def _():
                piece = weights[k].at[s, t, pl.ds(i * rb, rb)]
                remote(piece, piece, first_send.at[k, 0], first_recv.at[k, i], tp=other).wait_recv()

    reach = ((ns // 2, ns // 2 - 1), (ns // 2 - 1, ns // 2))

    def onward(k, slot, i, way, hop):
        piece = weights[k].at[slot, t, pl.ds(i * rb, rb)]
        return remote(
            piece, piece, z_send.at[k, way], z_recv.at[k, way, i, hop], sp=(s_next, s_prev)[way]
        )

    def across(k, slot, i):
        piece = weights[k].at[slot, t, pl.ds(i * rb, rb)]
        return remote(piece, piece, p_send.at[k], p_recv.at[k], tp=other)

    def launch(k):
        for i in range(2):
            for way in range(2):
                if reach[way][i] >= 1:
                    onward(k, s, i, way, 1).start()
        for i in range(2):
            across(k, s, i).start()

    def when(condition, body):
        if isinstance(condition, bool):
            if condition:
                body()
        else:
            pl.when(condition)(body)

    def ring_step(k, hop):
        for i in range(2):
            for way in range(2):
                slot = lax.rem(s + ns - hop, ns) if way == 0 else lax.rem(s + hop, ns)

                def body(slot=slot, i=i, way=way):
                    onward(k, slot, i, way, hop).wait_recv()
                    when(hop < reach[way][i], lambda: onward(k, slot, i, way, hop + 1).start())
                    across(k, slot, i).start()

                when(hop <= reach[way][i], body)

    def wait_across(k):
        piece = weights[k].at[:, other]
        remote(piece, piece, p_send.at[k], p_recv.at[k], tp=other).wait_recv()

    wait_first(0)
    launch(0)
    early = max(1, ns // 4)
    for hop in range(1, early):
        ring_step(0, hop)

    def x_block(which, part, way, kind):
        ref = x_all.at[which, halves[part]]
        return remote(ref, ref, x_send.at[way], x_recv.at[way, kind], fs=(f_next, f_prev)[way])

    x_block(f_prev, 0, 0, 0).wait_recv()
    x_block(f_prev, 0, 0, 2).start()
    x_block(f_next, 1, 1, 1).wait_recv()
    x_block(f_next, 1, 1, 2).start()
    for hop in range(early, ns // 2):
        ring_step(0, hop)
    wait_first(1)
    launch(1)
    ring_step(0, ns // 2)
    x_block(f_prev, 1, 0, 1).wait_recv()
    x_block(f_next, 0, 1, 0).wait_recv()
    x_block(f_far, 0, 0, 2).wait_recv()
    x_block(f_far, 1, 1, 2).wait_recv()
    wait_across(0)
    remote(aux_in, aux.at[other], aux_send, aux_recv, tp=other).wait_recv()

    def project(column, size):
        w = w_in[:, :, :, pl.ds(column, size)].reshape(width, size)
        a = x_all[...].reshape(nf * rows, width)
        return jnp.dot(a, w, preferred_element_type=F32).astype(BF16)

    kv_rows[:, WINDOW:, :] = project(4 * quarter, kvw).reshape(nf, rows, kvw)

    kv_src, kv_dst = kv_rows.at[:, pl.ds(rows, WINDOW)], kv_rows.at[:, pl.ds(0, WINDOW)]
    gated_src, gated_dst = gated.at[:, pl.ds(rows, 16)], gated.at[:, pl.ds(0, 16)]

    def send_halo(n, src, dst):
        @pl.when(t == 0)
        def _():
            remote(src, dst, halo_send.at[n], halo_recv.at[n], tp=1).start()

        @pl.when(t == 1)
        def _():
            remote(src, dst, halo_send.at[n], halo_recv.at[n], sp=s_next, tp=0).start()

    tiles = 4 * quarter // TILE

    def projection(n, carry):
        when(n < ns // 2, lambda: ring_step(1, n + 1))
        proj[n] = project(pl.multiple_of(n * TILE, TILE), TILE).reshape(nf, rows, TILE)
        return carry

    send_halo(0, kv_src, kv_dst)
    lax.fori_loop(0, tiles, projection, 0)
    for hop in range(tiles + 1, ns // 2 + 1):
        ring_step(1, hop)

    per = quarter // TILE

    def gate(q, carry):
        for n in range(per):
            g = proj[per + n, q].astype(F32) * proj[2 * per + n, q].astype(F32)
            gated[q, 16:, pl.ds(n * TILE, TILE)] = g.astype(BF16)
        return carry

    lax.fori_loop(0, nf, gate, 0)
    send_halo(1, gated_src, gated_dst)

    aux_here = aux.at[f // 2, lax.rem(f, 2)]
    at_start = jnp.logical_and(s == 0, t == 0)

    remote(kv_dst, kv_dst, halo_send.at[0], halo_recv.at[0], tp=other).wait_recv()
    key_id = lax.broadcasted_iota(jnp.int32, (WINDOW, 2 * WINDOW), 1)
    query_id = lax.broadcasted_iota(jnp.int32, (WINDOW, 2 * WINDOW), 0)
    low = lax.broadcasted_iota(jnp.int32, (2 * WINDOW, kvw), 1) < HEAD

    def attend(step, carry):
        q = step // blocks
        b = lax.rem(step, blocks)
        begin = pl.multiple_of(b * WINDOW, WINDOW)
        both = kv_rows[q, pl.ds(begin, 2 * WINDOW), :].astype(F32)
        turned = pltpu.roll(both, HEAD, 1)
        zero = jnp.zeros_like(both)
        keys = jnp.concatenate([jnp.where(low, both, zero), jnp.where(low, zero, turned)], 0).astype(BF16)
        values = jnp.concatenate([jnp.where(low, turned, zero), jnp.where(low, zero, both)], 0).astype(BF16)
        first_key = jnp.where(jnp.logical_and(at_start, b == 0), WINDOW, 0)
        allowed = (key_id > query_id) & (key_id <= query_id + WINDOW) & (key_id >= first_key)
        for pair in range(quarter // (2 * HEAD)):
            n, lane = pair * 2 * HEAD // TILE, pair * 2 * HEAD % TILE
            queries = proj[n, q, pl.ds(begin, WINDOW), lane : lane + 2 * HEAD]
            scores = rows_dot(queries, keys) * (1.0 / HEAD**0.5)
            probs = []
            for h in range(2):
                score = jnp.where(allowed, scores[:, h * 2 * WINDOW : (h + 1) * 2 * WINDOW], -jnp.inf)
                sink = aux_here[8 + 2 * pair + h : 9 + 2 * pair + h, 0:1]
                peak = jnp.maximum(jnp.max(score, axis=-1, keepdims=True), sink)
                weight = jnp.exp(score - peak)
                total = jnp.sum(weight, axis=-1, keepdims=True) + jnp.exp(sink - peak)
                probs.append((weight * (1.0 / total)).astype(BF16))
            attended = jnp.dot(jnp.concatenate(probs, 1), values, preferred_element_type=F32)
            acts[q, pl.ds(begin, WINDOW), quarter + pair * 2 * HEAD : quarter + (pair + 1) * 2 * HEAD] = attended.astype(BF16)
        return carry

    lax.fori_loop(0, nf * blocks, attend, 0)

    remote(gated_dst, gated_dst, halo_send.at[1], halo_recv.at[1], tp=other).wait_recv()

    @pl.when(at_start)
    def _():
        gated[:, 0:16, :] = jnp.zeros_like(gated[:, 0:16, :])

    def convolve(q, carry):
        for n in range(per):
            span = pl.ds(n * TILE, TILE)
            g = gated[q, :, span].astype(F32)
            taps = aux_here[0:TAPS, n * TILE : (n + 1) * TILE]
            total = pltpu.roll(g, 2, 0)[16:] * taps[0:1] + pltpu.roll(g, 1, 0)[16:] * taps[1:2] + g[16:] * taps[2:3]
            acts[q, :, span] = (proj[3 * per + n, q].astype(F32) * total).astype(BF16)
        return carry

    lax.fori_loop(0, nf, convolve, 0)

    wait_across(1)
    count = width // TILE
    near_half = count // 2
    chips = TILE // (2 * 2 * rb)

    def partial(q, n):
        w = w_out[pl.ds(n * chips, chips)].reshape(TILE, 2 * quarter)
        return rows_dot(acts[q], w)

    ways = ((f_next, f_prev), (f_prev, f_next))

    def far_copy(way, n):
        return remote(
            send_far.at[way, n], recv_far.at[way, n], far_send.at[way], far_recv.at[way, n], fs=ways[way][0]
        )

    def near_copy(way, n):
        return remote(
            send_near.at[way, n], recv_near.at[way, n], near_send.at[way], near_recv.at[way, n], fs=ways[way][0]
        )

    def far_step(n, carry):
        send_far[0, n] = partial(f_far, n).astype(BF16)
        send_far[1, n] = partial(f_far, n + near_half).astype(BF16)
        far_copy(0, n).start()
        far_copy(1, n).start()
        return carry

    def plain_step(n, carry):
        send_near[0, n + near_half] = partial(f_next, n + near_half).astype(BF16)
        send_near[1, n] = partial(f_prev, n).astype(BF16)
        near_copy(0, n + near_half).start()
        near_copy(1, n).start()
        return carry

    def joined_step(n, carry):
        first, second = partial(f_next, n), partial(f_prev, n + near_half)
        far_copy(0, n).wait_recv()
        far_copy(1, n).wait_recv()
        send_near[0, n] = (first + recv_far[0, n].astype(F32)).astype(BF16)
        send_near[1, n + near_half] = (second + recv_far[1, n].astype(F32)).astype(BF16)
        near_copy(0, n).start()
        near_copy(1, n + near_half).start()
        return carry

    def own_step(n, carry):
        own_sum[n] = partial(f, n)
        return carry

    lax.fori_loop(0, near_half, far_step, 0)
    lax.fori_loop(0, near_half, plain_step, 0)
    lax.fori_loop(0, near_half, joined_step, 0)
    lax.fori_loop(0, count, own_step, 0)
    for n in range(near_half):
        for way, tile in ((0, n + near_half), (1, n)):
            near_copy(way, tile).wait_recv()
    for n in range(near_half):
        for way, tile in ((0, n), (1, n + near_half)):
            near_copy(way, tile).wait_recv()
        for tile in (n, n + near_half):
            total = own_sum[tile] + recv_near[0, tile].astype(F32) + recv_near[1, tile].astype(F32)
            out[:, tile * TILE : (tile + 1) * TILE] = total.astype(BF16)

    for k in range(2):
        for j in range(2):
            here = jnp.logical_and(2 * t + j == f, mine == t)

            @pl.when(jnp.logical_not(here))
            def _():
                piece = weights[k].at[s, t, pl.ds(0, rb)]
                remote(piece, piece, first_send.at[k, j], first_recv.at[k, 0], tp=other).wait_send()

        for way in range(2):
            pieces = weights[k].at[pl.ds(0, ns - 1), 0, pl.ds(0, rb)]
            remote(pieces, pieces, z_send.at[k, way], z_recv.at[k, way, 0, 0], tp=other).wait_send()
        piece = weights[k].at[:, t]
        remote(piece, piece, p_send.at[k], p_recv.at[k], tp=other).wait_send()
    for way in range(2):
        ref = x_all.at[pl.ds(0, 3), halves[0]]
        remote(ref, ref, x_send.at[way], x_recv.at[way, 0], tp=other).wait_send()
        remote(send_far.at[way], send_far.at[way], far_send.at[way], far_recv.at[way, 0], tp=other).wait_send()
        remote(send_near.at[way], send_near.at[way], near_send.at[way], near_recv.at[way, 0], tp=other).wait_send()
    remote(aux_in, aux_in, aux_send, aux_recv, tp=other).wait_send()
    remote(kv_src, kv_src, halo_send.at[0], halo_recv.at[0], tp=other).wait_send()
    remote(gated_src, gated_src, halo_send.at[1], halo_recv.at[1], tp=other).wait_send()


def local(
    ns,
    nf,
    tokens,
    norm_gain,
    w_bgate,
    w_cgate,
    w_conv_in,
    conv_taps,
    w_query,
    w_key,
    w_value,
    sink_logits,
    conv_out_weight,
    attn_out_weight,
):
    widened = tokens[0].astype(F32)
    normed = (
        widened * lax.rsqrt(jnp.mean(widened * widened, axis=-1, keepdims=True) + EPSILON) * norm_gain
    ).astype(BF16)
    rows, width = normed.shape
    rb, columns = w_query.shape
    quarter = columns // 2
    kvw = w_key.shape[1]
    kv_pack = jnp.stack(
        [
            jnp.concatenate([w[:, j * HEAD : (j + 1) * HEAD] for w in (w_key, w_value)], axis=1)
            for j in range(2)
        ]
    )
    out_pack = jnp.concatenate(
        [jnp.swapaxes(w.reshape(2, quarter, rb), 1, 2) for w in (conv_out_weight, attn_out_weight)], axis=2
    )
    heads = quarter // HEAD
    taps = jnp.swapaxes(conv_taps.astype(F32).reshape(TAPS, 2, quarter), 0, 1)
    sinks = jnp.broadcast_to(sink_logits.reshape(2, heads, 1), (2, heads, quarter))
    aux = jnp.concatenate([jnp.pad(taps, ((0, 0), (0, 8 - TAPS), (0, 0))), sinks], axis=1)
    count = width // TILE
    vmem = pl.BlockSpec(memory_space=pltpu.VMEM)
    dma = pltpu.SemaphoreType.DMA
    inside = 4 * quarter + kvw
    out = pl.pallas_call(
        functools.partial(layer_kernel, ns, nf),
        out_shape=jax.ShapeDtypeStruct((rows, width), BF16),
        in_specs=[vmem] * 8,
        out_specs=vmem,
        scratch_shapes=[
            pltpu.VMEM((nf, rows, width), BF16),
            pltpu.VMEM((ns, 2, 2 * rb, inside), BF16),
            pltpu.VMEM((ns, 2, 2 * rb, 2 * quarter), BF16),
            pltpu.VMEM((4 * quarter // TILE, nf, rows, TILE), BF16),
            pltpu.VMEM((nf, WINDOW + rows, kvw), BF16),
            pltpu.VMEM((nf, 16 + rows, quarter), BF16),
            pltpu.VMEM((nf, rows, 2 * quarter), BF16),
            pltpu.VMEM((2, *aux.shape), F32),
            pltpu.VMEM((2, count // 2, rows, TILE), BF16),
            pltpu.VMEM((2, count // 2, rows, TILE), BF16),
            pltpu.VMEM((2, count, rows, TILE), BF16),
            pltpu.VMEM((2, count, rows, TILE), BF16),
            pltpu.VMEM((count, rows, TILE), F32),
            dma((2, 2)),
            dma((2, 2)),
            dma((2, 2)),
            dma((2, 2, 2, ns // 2 + 1)),
            dma((2,)),
            dma((2,)),
            dma((2,)),
            dma((2, 3)),
            dma,
            dma,
            dma((2,)),
            dma((2,)),
            dma((2,)),
            dma((2, count // 2)),
            dma((2,)),
            dma((2, count)),
        ],
        compiler_params=pltpu.CompilerParams(
            collective_id=0, has_side_effects=True, vmem_limit_bytes=62 * 1024 * 1024
        ),
        name="layer",
    )(normed, w_query, w_conv_in, w_cgate, w_bgate, kv_pack, out_pack, aux)
    return out[None]


def solution(mesh):
    placed = (
        P(("grp", "fs"), ("sp", "tp"), None),
        P(),
        P(("sp", "fs"), "tp"),
        P(("sp", "fs"), "tp"),
        P(("sp", "fs"), "tp"),
        P(None, "tp"),
        P(("sp", "fs"), "tp"),
        P(("sp", "fs"), "tp"),
        P(("sp", "fs"), "tp"),
        P("tp"),
        P("tp", ("sp", "fs")),
        P("tp", ("sp", "fs")),
    )
    return jax.shard_map(
        functools.partial(local, mesh.shape["sp"], mesh.shape["fs"]),
        mesh=mesh,
        in_specs=placed,
        out_specs=P(("grp", "fs"), ("sp", "tp"), None),
        check_vma=False,
    )
```

```python
import functools

import jax
import jax.numpy as jnp
from jax import lax
from jax.experimental import pallas as pl
from jax.experimental.pallas import tpu as pltpu
from jax.sharding import PartitionSpec as P

HEAD = 64
WINDOW = 128
TAPS = 3
EPSILON = 1e-06
MESH = pl.DeviceIdType.MESH
F32 = jnp.float32
BF16 = jnp.bfloat16
TILE = 256


def rows_dot(a, b):
    return lax.dot_general(a, b, (((1,), (1,)), ((), ())), preferred_element_type=F32)


def layer_kernel(
    ns,
    nf,
    tokens,
    gain,
    w_query,
    w_conv_in,
    w_cgate,
    w_bgate,
    w_key,
    w_value,
    conv_taps,
    sinks,
    conv_out,
    attn_out,
    out,
    x_all,
    w_in,
    w_out,
    kv_pack,
    proj,
    kv_rows,
    gated,
    acts,
    aux,
    sink_rows,
    send_far,
    recv_far,
    send_near,
    recv_near,
    own_sum,
    first_send,
    first_recv,
    z_send,
    z_recv,
    y_send,
    y_recv,
    p_send,
    p_recv,
    x_send,
    x_recv,
    aux_send,
    aux_recv,
    halo_send,
    halo_recv,
    far_send,
    far_recv,
    near_send,
    near_recv,
):
    g = lax.axis_index("grp")
    s = lax.axis_index("sp")
    f = lax.axis_index("fs")
    t = lax.axis_index("tp")
    odd = lax.rem(g, 2)
    pair = g + 1 - 2 * odd
    s_next, s_prev = lax.rem(s + 1, ns), lax.rem(s + ns - 1, ns)
    f_next, f_prev = lax.rem(f + 1, nf), lax.rem(f + nf - 1, nf)
    f_far = lax.rem(f + 2, nf)
    other = 1 - t
    rows, width = tokens.shape
    rb = w_query.shape[0]
    quarter = w_query.shape[1] // 2
    kvw = w_key.shape[1]
    half = rows // 2
    blocks = rows // WINDOW

    def remote(src, dst, send_sem, recv_sem, **where):
        return pltpu.make_async_remote_copy(
            src_ref=src,
            dst_ref=dst,
            send_sem=send_sem,
            recv_sem=recv_sem,
            device_id=where,
            device_id_type=MESH,
        )

    def when(condition, body):
        if isinstance(condition, bool):
            if condition:
                body()
        else:
            pl.when(condition)(body)

    barrier = pltpu.get_barrier_semaphore()
    greeted = [
        {"fs": lax.rem(f + df, nf), "tp": lax.rem(t + dt, 2)}
        for df in range(nf)
        for dt in range(2)
        if df or dt
    ]
    greeted += [{"sp": z, "tp": lax.rem(t + dt, 2)} for z in (s_next, s_prev) for dt in range(2)]
    greeted.append({"grp": pair})
    for device in greeted:
        pl.semaphore_signal(barrier, inc=1, device_id=device, device_id_type=MESH)

    with jax.named_scope("norm"):
        step_rows = 32

        def norm(r, carry):
            span = pl.ds(pl.multiple_of(r * step_rows, step_rows), step_rows)
            wide = tokens[span, :].astype(F32)
            scale = lax.rsqrt(jnp.mean(wide * wide, axis=-1, keepdims=True) + EPSILON)
            x_all[f, span, :] = (wide * scale * gain[...]).astype(BF16)
            return carry

        lax.fori_loop(0, rows // step_rows, norm, 0)
        low = lax.broadcasted_iota(jnp.int32, (rb, kvw), 1) < HEAD
        keys_wide, values_wide = w_key[...].astype(F32), w_value[...].astype(F32)
        kv_pack[0] = jnp.where(low, keys_wide, pltpu.roll(values_wide, HEAD, 1)).astype(BF16)
        kv_pack[1] = jnp.where(low, pltpu.roll(keys_wide, HEAD, 1), values_wide).astype(BF16)
        aux[t, 0:TAPS, :] = conv_taps[...].astype(F32)
        aux[t, 8:9, 0 : sinks.shape[1]] = sinks[...]
    with jax.named_scope("meet"):
        pl.semaphore_wait(barrier, len(greeted))

    y_in, y_out = 3 * quarter // 2, quarter // 2
    z_in, z_out = y_in + quarter + kvw, 3 * quarter // 2
    weights = (w_in, w_out)
    lane = pl.multiple_of
    z_span = (pl.ds(lane(odd * y_in, 128), z_in), pl.ds(lane(odd * y_out, 128), z_out))
    y_span = (pl.ds(lane(odd * z_in, 128), y_in), pl.ds(lane(odd * z_out, 128), y_out))
    y_other = (pl.ds(lane((1 - odd) * z_in, 128), y_in), pl.ds(lane((1 - odd) * z_out, 128), y_out))
    mid = quarter // 2

    mine = f // 2
    first = lax.rem(f, 2)
    slot_rows = pl.ds(pl.multiple_of(first * rb, rb), rb)
    for k in range(2):
        for j in range(2):
            to_f = 2 * t + j
            here = jnp.logical_and(to_f == f, mine == t)
            base = j * quarter
            if k == 0:
                common = [(w_query, base, y_in, quarter), (kv_pack, None, y_in + quarter, kvw)]
                shares = (
                    [(w_conv_in, base, 0, quarter), (w_cgate, base, quarter, mid)],
                    [(w_cgate, base + mid, z_in, mid), (w_bgate, base, z_in + mid, quarter)],
                )
            else:
                common = []
                shares = (
                    [(conv_out, base, 0, quarter), (attn_out, base, quarter, mid)],
                    [(conv_out, base + mid, mid, mid), (attn_out, base, quarter, quarter)],
                )

            def deliver(moves, here=here, to_f=to_f, j=j, k=k):
                def ends(move):
                    ref, start, column, size = move
                    src = ref.at[j] if start is None else ref.at[:, pl.ds(start, size)]
                    return src, weights[k].at[s, mine, slot_rows, pl.ds(column, size)]

                @pl.when(jnp.logical_not(here))
                def _():
                    for move in moves:
                        src, dst = ends(move)
                        remote(src, dst, first_send.at[k, j], first_recv.at[k, first], fs=to_f, tp=mine).start()

                @pl.when(here)
                def _():
                    for move in moves:
                        src, dst = ends(move)
                        dst[...] = src[...]

            if common:
                deliver(common)
            for parity in range(2):
                pl.when(odd == parity)(functools.partial(deliver, shares[parity]))
        if k == 0:
            halves = (pl.ds(0, half), pl.ds(half, half))
            for which in (0, 1):
                for way, part, to in ((0, which, f_next), (1, 1 - which, f_prev)):
                    ref = x_all.at[f, halves[part]]
                    remote(ref, ref, x_send.at[way], x_recv.at[way, part], fs=to).start()
    remote(aux.at[t], aux.at[t], aux_send, aux_recv, tp=other).start()

    def wait_first(k):
        for i in range(2):
            local = jnp.logical_and(t == f // 2, f == 2 * t + i)

            @pl.when(jnp.logical_not(local))
            def _():
                piece = weights[k].at[s, t, pl.ds(i * rb, rb), z_span[k]]
                remote(piece, piece, first_send.at[k, 0], first_recv.at[k, i], tp=other).wait_recv()

    reach = ((ns // 2, ns // 2 - 1), (ns // 2 - 1, ns // 2))

    def onward(k, slot, i, way, hop):
        piece = weights[k].at[slot, t, pl.ds(i * rb, rb), z_span[k]]
        return remote(
            piece, piece, z_send.at[k, way], z_recv.at[k, way, i, hop], sp=(s_next, s_prev)[way]
        )

    def across(k, slot, i):
        piece = weights[k].at[slot, t, pl.ds(i * rb, rb), z_span[k]]
        return remote(piece, piece, p_send.at[0, k], p_recv.at[0, k], tp=other)

    def to_pair(k, slot, i, way, hop):
        piece = weights[k].at[slot, t, pl.ds(i * rb, rb), y_span[k]]
        return remote(piece, piece, y_send.at[k], y_recv.at[k, way, i, hop], grp=pair)

    def from_pair(k, slot, i, way, hop):
        piece = weights[k].at[slot, t, pl.ds(i * rb, rb), y_other[k]]
        remote(piece, piece, y_send.at[k], y_recv.at[k, way, i, hop], grp=pair).wait_recv()
        remote(piece, piece, p_send.at[1, k], p_recv.at[1, k], tp=other).start()

    def launch(k):
        for i in range(2):
            for way in range(2):
                if reach[way][i] >= 1:
                    onward(k, s, i, way, 1).start()
            to_pair(k, s, i, 0, 0).start()
        for i in range(2):
            across(k, s, i).start()

    def slot_of(way, hop):
        return lax.rem(s + ns - hop, ns) if way == 0 else lax.rem(s + hop, ns)

    def ring_step(k, hop):
        for i in range(2):
            for way in range(2):

                def body(slot=slot_of(way, hop), i=i, way=way):
                    onward(k, slot, i, way, hop).wait_recv()
                    when(hop < reach[way][i], lambda: onward(k, slot, i, way, hop + 1).start())
                    to_pair(k, slot, i, way, hop).start()
                    across(k, slot, i).start()

                when(hop <= reach[way][i], body)

    def pair_step(k, hop):
        for i in range(2):
            for way in range(2):
                body = functools.partial(from_pair, k, slot_of(way, hop), i, way, hop)
                if way == 0:
                    when(hop <= reach[way][i], body)
                elif isinstance(hop, int):
                    when(0 < hop <= reach[way][i], body)
                else:
                    when(jnp.logical_and(hop > 0, hop <= reach[way][i]), body)

    def wait_across(k):
        for n, span in ((0, z_span), (1, y_other)):
            piece = weights[k].at[:, other, :, span[k]]
            remote(piece, piece, p_send.at[n, k], p_recv.at[n, k], tp=other).wait_recv()

    last = ns // 2
    with jax.named_scope("first_wait"):
        wait_first(0)
    launch(0)
    early = max(1, ns // 4)
    with jax.named_scope("ring0_early"):
        for hop in range(1, early):
            ring_step(0, hop)
            if hop >= 2:
                pair_step(0, hop - 2)

    def x_block(which, part, way, kind):
        ref = x_all.at[which, halves[part]]
        return remote(ref, ref, x_send.at[way], x_recv.at[way, kind], fs=(f_next, f_prev)[way])

    with jax.named_scope("rows_onward"):
        x_block(f_prev, 0, 0, 0).wait_recv()
        x_block(f_prev, 0, 0, 2).start()
        x_block(f_next, 1, 1, 1).wait_recv()
        x_block(f_next, 1, 1, 2).start()
    with jax.named_scope("ring0_late"):
        for hop in range(early, last + 1):
            ring_step(0, hop)
            if hop >= 2:
                pair_step(0, hop - 2)
            if hop == max(last - 2, early):
                wait_first(1)
                launch(1)
    with jax.named_scope("pair_late"):
        for hop in range(max(last - 1, 0), last + 1):
            pair_step(0, hop)
            if hop == last - 1:
                ring_step(1, 1)
    with jax.named_scope("rows_wait"):
        x_block(f_prev, 1, 0, 1).wait_recv()
        x_block(f_next, 0, 1, 0).wait_recv()
        x_block(f_far, 0, 0, 2).wait_recv()
        x_block(f_far, 1, 1, 2).wait_recv()
    with jax.named_scope("across0"):
        wait_across(0)
    remote(aux.at[other], aux.at[other], aux_send, aux_recv, tp=other).wait_recv()

    def project(column, size):
        w = w_in[:, :, :, pl.ds(column, size)].reshape(width, size)
        a = x_all[...].reshape(nf * rows, width)
        return jnp.dot(a, w, preferred_element_type=F32).astype(BF16)

    with jax.named_scope("project_kv"):
        kv_rows[:, WINDOW:, :] = project(y_in + quarter, kvw).reshape(nf, rows, kvw)

    kv_src, kv_dst = kv_rows.at[:, pl.ds(rows, WINDOW)], kv_rows.at[:, pl.ds(0, WINDOW)]
    gated_src, gated_dst = gated.at[:, pl.ds(rows, 16)], gated.at[:, pl.ds(0, 16)]

    def send_halo(n, src, dst):
        @pl.when(t == 0)
        def _():
            remote(src, dst, halo_send.at[n], halo_recv.at[n], tp=1).start()

        @pl.when(t == 1)
        def _():
            remote(src, dst, halo_send.at[n], halo_recv.at[n], sp=s_next, tp=0).start()

    tiles = 4 * quarter // TILE

    def projection(n, carry):
        column = pl.multiple_of(n * TILE + n // 5 * kvw, 128)
        pl.when(n + 2 <= last)(lambda: ring_step(1, n + 2))
        pl.when(n <= last)(lambda: pair_step(1, n))
        proj[n] = project(column, TILE).reshape(nf, rows, TILE)
        return carry

    send_halo(0, kv_src, kv_dst)
    with jax.named_scope("projections"):
        lax.fori_loop(0, tiles, projection, 0)
        for hop in range(tiles + 2, last + 1):
            ring_step(1, hop)

    per = quarter // TILE

    def gate(q, carry):
        for n in range(per):
            product = proj[n, q].astype(F32) * proj[(2, 5)[n], q].astype(F32)
            gated[q, 16:, pl.ds(n * TILE, TILE)] = product.astype(BF16)
        return carry

    with jax.named_scope("gates"):
        lax.fori_loop(0, nf, gate, 0)
        aux_lane = lax.broadcasted_iota(jnp.int32, (1, 128), 1)
        heads = quarter // HEAD
        held = aux[f // 2, 8:9, 0:128]
        for h in range(heads):
            one = jnp.sum(jnp.where(aux_lane == first * heads + h, held, 0.0), axis=-1, keepdims=True)
            sink_rows[h : h + 1, :] = jnp.broadcast_to(one * HEAD**0.5, (1, 128))
    send_halo(1, gated_src, gated_dst)

    at_start = jnp.logical_and(s == 0, t == 0)

    key_id = lax.broadcasted_iota(jnp.int32, (2 * WINDOW, WINDOW), 0)
    query_id = lax.broadcasted_iota(jnp.int32, (2 * WINDOW, WINDOW), 1)
    low_keys = lax.broadcasted_iota(jnp.int32, (2 * WINDOW, kvw), 1) < HEAD

    def attend(step, carry):
        q = step // blocks
        b = lax.rem(step, blocks)
        begin = pl.multiple_of(b * WINDOW, WINDOW)
        both = kv_rows[q, pl.ds(begin, 2 * WINDOW), :].astype(F32)
        turned = pltpu.roll(both, HEAD, 1)
        zero = jnp.zeros_like(both)
        keys = jnp.concatenate([jnp.where(low_keys, both, zero), jnp.where(low_keys, zero, turned)], 0).astype(BF16)
        values = jnp.concatenate([jnp.where(low_keys, turned, zero), jnp.where(low_keys, zero, both)], 0)
        values = jnp.transpose(values).astype(BF16)
        first_key = jnp.where(jnp.logical_and(at_start, b == 0), WINDOW, 0)
        allowed = (key_id > query_id) & (key_id <= query_id + WINDOW) & (key_id >= first_key)
        for duo in range(quarter // (2 * HEAD)):
            n, column = 3 + duo * 2 * HEAD // TILE, duo * 2 * HEAD % TILE
            queries = proj[n, q, pl.ds(begin, WINDOW), column : column + 2 * HEAD]
            scores = rows_dot(keys, queries)
            probs = []
            for h in range(2):
                score = jnp.where(allowed, scores[h * 2 * WINDOW : (h + 1) * 2 * WINDOW], -jnp.inf)
                sink = sink_rows[2 * duo + h : 2 * duo + h + 1, :]
                peak = jnp.maximum(jnp.max(score, axis=0, keepdims=True), sink)
                weight = jnp.exp((score - peak) * (1.0 / HEAD**0.5))
                total = jnp.sum(weight, axis=0, keepdims=True) + jnp.exp((sink - peak) * (1.0 / HEAD**0.5))
                probs.append((weight * (1.0 / total)).astype(BF16))
            attended = jnp.dot(values, jnp.concatenate(probs, 0), preferred_element_type=F32)
            span = pl.ds(quarter + duo * 2 * HEAD, 2 * HEAD)
            acts[q, pl.ds(begin, WINDOW), span] = jnp.transpose(attended).astype(BF16)
        return carry

    with jax.named_scope("halo_wait"):
        remote(kv_dst, kv_dst, halo_send.at[0], halo_recv.at[0], tp=other).wait_recv()
    with jax.named_scope("attention"):
        lax.fori_loop(0, nf * blocks, attend, 0)

    remote(gated_dst, gated_dst, halo_send.at[1], halo_recv.at[1], tp=other).wait_recv()

    @pl.when(at_start)
    def _():
        gated[:, 0:16, :] = jnp.zeros_like(gated[:, 0:16, :])

    def convolve(q, carry):
        for n in range(per):
            span = pl.ds(n * TILE, TILE)
            wide = gated[q, :, span].astype(F32)
            taps = aux[f // 2, 0:TAPS, pl.ds(pl.multiple_of(first * quarter + n * TILE, TILE), TILE)]
            total = (
                pltpu.roll(wide, 2, 0)[16:] * taps[0:1]
                + pltpu.roll(wide, 1, 0)[16:] * taps[1:2]
                + wide[16:] * taps[2:3]
            )
            acts[q, :, span] = (proj[6 + n, q].astype(F32) * total).astype(BF16)
        return carry

    with jax.named_scope("convolution"):
        lax.fori_loop(0, nf, convolve, 0)

    with jax.named_scope("across1"):
        for hop in range(tiles, last + 1):
            pair_step(1, hop)
        wait_across(1)
    count = width // TILE
    near_half = count // 2
    chips = TILE // (2 * 2 * rb)

    def partial(q, n):
        w = w_out[pl.ds(n * chips, chips)].reshape(TILE, 2 * quarter)
        return rows_dot(acts[q], w)

    ways = (f_next, f_prev)

    def far_copy(way, n):
        return remote(send_far.at[way, n], recv_far.at[way, n], far_send.at[way], far_recv.at[way, n], fs=ways[way])

    def near_copy(way, n):
        return remote(
            send_near.at[way, n], recv_near.at[way, n], near_send.at[way], near_recv.at[way, n], fs=ways[way]
        )

    def far_step(n, carry):
        send_far[0, n] = partial(f_far, n).astype(BF16)
        send_far[1, n] = partial(f_far, n + near_half).astype(BF16)
        far_copy(0, n).start()
        far_copy(1, n).start()
        return carry

    def plain_step(n, carry):
        send_near[0, n + near_half] = partial(f_next, n + near_half).astype(BF16)
        send_near[1, n] = partial(f_prev, n).astype(BF16)
        near_copy(0, n + near_half).start()
        near_copy(1, n).start()
        return carry

    def joined_step(n, carry):
        right, left = partial(f_next, n), partial(f_prev, n + near_half)
        far_copy(0, n).wait_recv()
        far_copy(1, n).wait_recv()
        send_near[0, n] = (right + recv_far[0, n].astype(F32)).astype(BF16)
        send_near[1, n + near_half] = (left + recv_far[1, n].astype(F32)).astype(BF16)
        near_copy(0, n).start()
        near_copy(1, n + near_half).start()
        return carry

    def own_step(n, carry):
        own_sum[n] = partial(f, n)
        return carry

    with jax.named_scope("far"):
        lax.fori_loop(0, near_half, far_step, 0)
    with jax.named_scope("plain"):
        lax.fori_loop(0, near_half, plain_step, 0)
    with jax.named_scope("joined"):
        lax.fori_loop(0, near_half, joined_step, 0)
    with jax.named_scope("own"):
        lax.fori_loop(0, count, own_step, 0)
    with jax.named_scope("finish"):
        for n in range(near_half):
            for way, tile in ((0, n + near_half), (1, n)):
                near_copy(way, tile).wait_recv()
        for n in range(near_half):
            for way, tile in ((0, n), (1, n + near_half)):
                near_copy(way, tile).wait_recv()
            for tile in (n, n + near_half):
                total = own_sum[tile] + recv_near[0, tile].astype(F32) + recv_near[1, tile].astype(F32)
                out[:, tile * TILE : (tile + 1) * TILE] = total.astype(BF16)

    for k in range(2):
        for j in range(2):
            here = jnp.logical_and(2 * t + j == f, mine == t)

            @pl.when(jnp.logical_not(here))
            def _():
                piece = weights[k].at[s, t, pl.ds(0, rb), z_span[k]]
                remote(piece, piece, first_send.at[k, j], first_recv.at[k, 0], tp=other).wait_send()

        for way in range(2):
            pieces = weights[k].at[pl.ds(0, ns - 1), 0, pl.ds(0, rb), z_span[k]]
            remote(pieces, pieces, z_send.at[k, way], z_recv.at[k, way, 0, 0], tp=other).wait_send()
        for n, span in ((0, z_span), (1, y_other)):
            piece = weights[k].at[:, t, :, span[k]]
            remote(piece, piece, p_send.at[n, k], p_recv.at[n, k], tp=other).wait_send()
        piece = weights[k].at[:, t, :, y_span[k]]
        remote(piece, piece, y_send.at[k], y_recv.at[k, 0, 0, 0], tp=other).wait_send()
    for way in range(2):
        ref = x_all.at[pl.ds(0, 3), halves[0]]
        remote(ref, ref, x_send.at[way], x_recv.at[way, 0], tp=other).wait_send()
        remote(send_far.at[way], send_far.at[way], far_send.at[way], far_recv.at[way, 0], tp=other).wait_send()
        remote(send_near.at[way], send_near.at[way], near_send.at[way], near_recv.at[way, 0], tp=other).wait_send()
    remote(aux.at[t], aux.at[t], aux_send, aux_recv, tp=other).wait_send()
    remote(kv_src, kv_src, halo_send.at[0], halo_recv.at[0], tp=other).wait_send()
    remote(gated_src, gated_src, halo_send.at[1], halo_recv.at[1], tp=other).wait_send()


def local(
    ns,
    nf,
    tokens,
    norm_gain,
    w_bgate,
    w_cgate,
    w_conv_in,
    conv_taps,
    w_query,
    w_key,
    w_value,
    sink_logits,
    conv_out_weight,
    attn_out_weight,
):
    rows, width = tokens.shape[1:]
    rb, columns = w_query.shape
    quarter = columns // 2
    kvw = w_key.shape[1]
    count = width // TILE
    inside = 4 * quarter + kvw
    vmem = pl.BlockSpec(memory_space=pltpu.VMEM)
    dma = pltpu.SemaphoreType.DMA
    out = pl.pallas_call(
        functools.partial(layer_kernel, ns, nf),
        out_shape=jax.ShapeDtypeStruct((rows, width), BF16),
        in_specs=[vmem] * 12,
        out_specs=vmem,
        scratch_shapes=[
            pltpu.VMEM((nf, rows, width), BF16),
            pltpu.VMEM((ns, 2, 2 * rb, inside), BF16),
            pltpu.VMEM((ns, 2, 2 * rb, 2 * quarter), BF16),
            pltpu.VMEM((2, rb, kvw), BF16),
            pltpu.VMEM((4 * quarter // TILE, nf, rows, TILE), BF16),
            pltpu.VMEM((nf, WINDOW + rows, kvw), BF16),
            pltpu.VMEM((nf, 16 + rows, quarter), BF16),
            pltpu.VMEM((nf, rows, 2 * quarter), BF16),
            pltpu.VMEM((2, 16, columns), F32),
            pltpu.VMEM((quarter // HEAD, 128), F32),
            pltpu.VMEM((2, count // 2, rows, TILE), BF16),
            pltpu.VMEM((2, count // 2, rows, TILE), BF16),
            pltpu.VMEM((2, count, rows, TILE), BF16),
            pltpu.VMEM((2, count, rows, TILE), BF16),
            pltpu.VMEM((count, rows, TILE), F32),
            dma((2, 2)),
            dma((2, 2)),
            dma((2, 2)),
            dma((2, 2, 2, ns // 2 + 1)),
            dma((2,)),
            dma((2, 2, 2, ns // 2 + 1)),
            dma((2, 2)),
            dma((2, 2)),
            dma((2,)),
            dma((2, 3)),
            dma,
            dma,
            dma((2,)),
            dma((2,)),
            dma((2,)),
            dma((2, count // 2)),
            dma((2,)),
            dma((2, count)),
        ],
        compiler_params=pltpu.CompilerParams(
            collective_id=0, has_side_effects=True, vmem_limit_bytes=62 * 1024 * 1024
        ),
        name="layer",
    )(
        tokens[0],
        norm_gain[None],
        w_query,
        w_conv_in,
        w_cgate,
        w_bgate,
        w_key,
        w_value,
        conv_taps,
        sink_logits[None],
        conv_out_weight.T,
        attn_out_weight.T,
    )
    return out[None]


def solution(mesh):
    placed = (
        P(("grp", "fs"), ("sp", "tp"), None),
        P(),
        P(("sp", "fs"), "tp"),
        P(("sp", "fs"), "tp"),
        P(("sp", "fs"), "tp"),
        P(None, "tp"),
        P(("sp", "fs"), "tp"),
        P(("sp", "fs"), "tp"),
        P(("sp", "fs"), "tp"),
        P("tp"),
        P("tp", ("sp", "fs")),
        P("tp", ("sp", "fs")),
    )
    return jax.shard_map(
        functools.partial(local, mesh.shape["sp"], mesh.shape["fs"]),
        mesh=mesh,
        in_specs=placed,
        out_specs=P(("grp", "fs"), ("sp", "tp"), None),
        check_vma=False,
    )
```

```python
import functools

import jax
import jax.numpy as jnp
from jax import lax
from jax.experimental import pallas as pl
from jax.experimental.pallas import tpu as pltpu
from jax.sharding import PartitionSpec as P

HEAD = 64
WINDOW = 128
TAPS = 3
EPSILON = 1e-06
MESH = pl.DeviceIdType.MESH
F32 = jnp.float32
BF16 = jnp.bfloat16
TILE = 256


def rows_dot(a, b):
    return lax.dot_general(a, b, (((1,), (1,)), ((), ())), preferred_element_type=F32)


def layer_kernel(
    ns,
    nf,
    *refs,
):
    given, out, held, rest = refs[:12], refs[12], refs[13:25], refs[25:]
    tokens, gain, w_query, w_conv_in, w_cgate, w_bgate, w_key, w_value, conv_taps, sinks, conv_out, attn_out = held
    (
        x_all,
        w_in,
        w_out,
        kv_pack,
        proj,
        kv_rows,
        gated,
        acts,
        aux,
        sink_rows,
        send_far,
        recv_far,
        send_near,
        recv_near,
        own_sum,
        first_send,
        first_recv,
        z_send,
        z_recv,
        y_send,
        y_recv,
        p_send,
        p_recv,
        x_send,
        x_recv,
        aux_send,
        aux_recv,
        halo_send,
        halo_recv,
        far_send,
        far_recv,
        near_send,
        near_recv,
        load_sem,
    ) = rest
    g = lax.axis_index("grp")
    s = lax.axis_index("sp")
    f = lax.axis_index("fs")
    t = lax.axis_index("tp")
    odd = lax.rem(g, 2)
    pair = g + 1 - 2 * odd
    s_next, s_prev = lax.rem(s + 1, ns), lax.rem(s + ns - 1, ns)
    f_next, f_prev = lax.rem(f + 1, nf), lax.rem(f + nf - 1, nf)
    f_far = lax.rem(f + 2, nf)
    other = 1 - t

    def seat(q):
        return lax.rem(q, 2) * 2 + q // 2

    mine_seat, far_seat, next_seat, prev_seat = seat(f), seat(f_far), seat(f_next), seat(f_prev)
    rows, width = tokens.shape
    rb = w_query.shape[0]
    quarter = w_query.shape[1] // 2
    kvw = w_key.shape[1]
    half = rows // 2
    blocks = rows // WINDOW

    def remote(src, dst, send_sem, recv_sem, **where):
        return pltpu.make_async_remote_copy(
            src_ref=src,
            dst_ref=dst,
            send_sem=send_sem,
            recv_sem=recv_sem,
            device_id=where,
            device_id_type=MESH,
        )

    loads = [pltpu.make_async_copy(a, b, load_sem.at[n]) for n, (a, b) in enumerate(zip(given, held))]
    for n in (*range(1, len(loads)), 0):
        loads[n].start()

    def when(condition, body):
        if isinstance(condition, bool):
            if condition:
                body()
        else:
            pl.when(condition)(body)

    barrier = pltpu.get_barrier_semaphore()
    greeted = [
        {"fs": lax.rem(f + df, nf), "tp": lax.rem(t + dt, 2)}
        for df in range(nf)
        for dt in range(2)
        if df or dt
    ]
    greeted += [{"sp": z, "tp": lax.rem(t + dt, 2)} for z in (s_next, s_prev) for dt in range(2)]
    greeted.append({"grp": pair})
    for device in greeted:
        pl.semaphore_signal(barrier, inc=1, device_id=device, device_id_type=MESH)

    with jax.named_scope("pack"):
        for load in loads[1:]:
            load.wait()
        low = lax.broadcasted_iota(jnp.int32, (rb, kvw), 1) < HEAD
        keys_wide, values_wide = w_key[...].astype(F32), w_value[...].astype(F32)
        kv_pack[0] = jnp.where(low, keys_wide, pltpu.roll(values_wide, HEAD, 1)).astype(BF16)
        kv_pack[1] = jnp.where(low, pltpu.roll(keys_wide, HEAD, 1), values_wide).astype(BF16)
        aux[t, 0:TAPS, :] = conv_taps[...].astype(F32)
        aux[t, 8:9, 0 : sinks.shape[1]] = sinks[...]
    with jax.named_scope("meet"):
        pl.semaphore_wait(barrier, len(greeted))

    y_in, y_out = 3 * quarter // 2, quarter // 2
    z_in, z_out = y_in + quarter + kvw, 3 * quarter // 2
    weights = (w_in, w_out)
    lane = pl.multiple_of
    z_span = (pl.ds(lane(odd * y_in, 128), z_in), pl.ds(lane(odd * y_out, 128), z_out))
    y_span = (pl.ds(lane(odd * z_in, 128), y_in), pl.ds(lane(odd * z_out, 128), y_out))
    y_other = (pl.ds(lane((1 - odd) * z_in, 128), y_in), pl.ds(lane((1 - odd) * z_out, 128), y_out))
    mid = quarter // 2

    mine = f // 2
    first = lax.rem(f, 2)
    slot_rows = pl.ds(pl.multiple_of(first * rb, rb), rb)
    def first_exchange(k):
        for j in range(2):
            to_f = 2 * t + j
            here = jnp.logical_and(to_f == f, mine == t)
            base = j * quarter
            if k == 0:
                common = [(w_query, base, y_in, quarter), (kv_pack, None, y_in + quarter, kvw)]
                shares = (
                    [(w_conv_in, base, 0, quarter), (w_cgate, base, quarter, mid)],
                    [(w_cgate, base + mid, z_in, mid), (w_bgate, base, z_in + mid, quarter)],
                )
            else:
                common = []
                shares = (
                    [(conv_out, base, 0, quarter), (attn_out, base, quarter, mid)],
                    [(conv_out, base + mid, mid, mid), (attn_out, base, quarter, quarter)],
                )

            def deliver(moves, here=here, to_f=to_f, j=j, k=k):
                def ends(move):
                    ref, start, column, size = move
                    src = ref.at[j] if start is None else ref.at[:, pl.ds(start, size)]
                    return src, weights[k].at[s, mine, slot_rows, pl.ds(column, size)]

                @pl.when(jnp.logical_not(here))
                def _():
                    for move in moves:
                        src, dst = ends(move)
                        remote(src, dst, first_send.at[k, j], first_recv.at[k, first], fs=to_f, tp=mine).start()

                @pl.when(here)
                def _():
                    for move in moves:
                        src, dst = ends(move)
                        dst[...] = src[...]

            if common:
                deliver(common)
            for parity in range(2):
                pl.when(odd == parity)(functools.partial(deliver, shares[parity]))

    first_exchange(0)
    with jax.named_scope("norm"):
        loads[0].wait()
        step_rows = 32

        def norm(r, carry):
            span = pl.ds(pl.multiple_of(r * step_rows, step_rows), step_rows)
            wide = tokens[span, :].astype(F32)
            scale = lax.rsqrt(jnp.mean(wide * wide, axis=-1, keepdims=True) + EPSILON)
            x_all[mine_seat, span, :] = (wide * scale * gain[...]).astype(BF16)
            return carry

        lax.fori_loop(0, rows // step_rows, norm, 0)
    remote(aux.at[t], aux.at[t], aux_send, aux_recv, tp=other).start()

    def wait_first(k):
        for i in range(2):
            local = jnp.logical_and(t == f // 2, f == 2 * t + i)

            @pl.when(jnp.logical_not(local))
            def _():
                piece = weights[k].at[s, t, pl.ds(i * rb, rb), z_span[k]]
                remote(piece, piece, first_send.at[k, 0], first_recv.at[k, i], tp=other).wait_recv()

    reach = ((ns // 2, ns // 2 - 1), (ns // 2 - 1, ns // 2))

    def onward(k, slot, i, way, hop):
        piece = weights[k].at[slot, t, pl.ds(i * rb, rb), z_span[k]]
        return remote(
            piece, piece, z_send.at[k, way], z_recv.at[k, way, i, hop], sp=(s_next, s_prev)[way]
        )

    def across(k, slot, i):
        piece = weights[k].at[slot, t, pl.ds(i * rb, rb), z_span[k]]
        return remote(piece, piece, p_send.at[0, k], p_recv.at[0, k], tp=other)

    def to_pair(k, slot, i, way, hop):
        piece = weights[k].at[slot, t, pl.ds(i * rb, rb), y_span[k]]
        return remote(piece, piece, y_send.at[k], y_recv.at[k, way, i, hop], grp=pair)

    def from_pair(k, slot, i, way, hop):
        piece = weights[k].at[slot, t, pl.ds(i * rb, rb), y_other[k]]
        remote(piece, piece, y_send.at[k], y_recv.at[k, way, i, hop], grp=pair).wait_recv()
        remote(piece, piece, p_send.at[1, k], p_recv.at[1, k], tp=other).start()

    def launch(k):
        for i in range(2):
            for way in range(2):
                if reach[way][i] >= 1:
                    onward(k, s, i, way, 1).start()
            to_pair(k, s, i, 0, 0).start()
        for i in range(2):
            across(k, s, i).start()

    def slot_of(way, hop):
        return lax.rem(s + ns - hop, ns) if way == 0 else lax.rem(s + hop, ns)

    def ring_part(k, hop, i):
        for way in range(2):

            def body(slot=slot_of(way, hop), way=way):
                onward(k, slot, i, way, hop).wait_recv()
                when(hop < reach[way][i], lambda: onward(k, slot, i, way, hop + 1).start())
                to_pair(k, slot, i, way, hop).start()
                across(k, slot, i).start()

            when(hop <= reach[way][i], body)

    def pair_part(k, hop, i):
        for way in range(2):
            body = functools.partial(from_pair, k, slot_of(way, hop), i, way, hop)
            if isinstance(hop, int):
                when(way <= hop <= reach[way][i], body)
            else:
                when(jnp.logical_and(hop >= way, hop <= reach[way][i]), body)

    def ring_step(k, hop):
        for i in range(2):
            ring_part(k, hop, i)

    def pair_step(k, hop):
        for i in range(2):
            pair_part(k, hop, i)

    lag = 2

    def ring_half(k, u):
        hop = u // 2
        for i in range(2):

            @pl.when(lax.rem(u, 2) == i)
            def _():
                pl.when(jnp.logical_and(hop >= 1, hop <= last))(lambda: ring_part(k, hop, i))
                pl.when(jnp.logical_and(hop >= lag, hop <= last + lag))(lambda: pair_part(k, hop - lag, i))

    last = ns // 2

    def wait_across(k):
        for n, span in ((0, z_span), (1, y_other)):
            piece = weights[k].at[:, other, :, span[k]]
            remote(piece, piece, p_send.at[n, k], p_recv.at[n, k], tp=other).wait_recv()

    with jax.named_scope("first_wait"):
        wait_first(0)
    launch(0)
    halves = (pl.ds(0, half), pl.ds(half, half))
    for which in (0, 1):
        for way, part, to in ((0, which, f_next), (1, 1 - which, f_prev)):
            ref = x_all.at[mine_seat, halves[part]]
            remote(ref, ref, x_send.at[way], x_recv.at[way, part], fs=to).start()
    first_exchange(1)
    early = max(1, ns // 4)
    start_out = max(last - 2, early)
    ahead = min(1, start_out - 1)
    resume = 2 * (last - start_out + ahead + 1)
    with jax.named_scope("ring0_early"):
        for hop in range(1, early):
            ring_step(0, hop)
            if hop >= 2:
                pair_step(0, hop - 2)

    def x_block(which, part, way, kind):
        ref = x_all.at[which, halves[part]]
        return remote(ref, ref, x_send.at[way], x_recv.at[way, kind], fs=(f_next, f_prev)[way])

    with jax.named_scope("rows_onward"):
        x_block(prev_seat, 0, 0, 0).wait_recv()
        x_block(prev_seat, 0, 0, 2).start()
        x_block(next_seat, 1, 1, 1).wait_recv()
        x_block(next_seat, 1, 1, 2).start()
    with jax.named_scope("ring0_late"):
        for hop in range(early, last + 1):
            ring_step(0, hop)
            if hop >= 2:
                pair_step(0, hop - 2)
            if hop == start_out:
                wait_first(1)
                launch(1)
            if hop > start_out:
                ring_step(1, hop - start_out)
    with jax.named_scope("pair_late"):
        for hop in range(max(last - 1, 0), last + 1):
            pair_step(0, hop)
            if 1 <= hop + ahead - last <= ahead:
                ring_step(1, last - start_out + hop + ahead - last)
        for hop in range(0, max(resume // 2 - lag, 0)):
            pair_step(1, hop)
    with jax.named_scope("rows_wait"):
        x_block(prev_seat, 1, 0, 1).wait_recv()
        x_block(next_seat, 0, 1, 0).wait_recv()
        x_block(far_seat, 0, 0, 2).wait_recv()
        x_block(far_seat, 1, 1, 2).wait_recv()
    with jax.named_scope("across0"):
        wait_across(0)
    remote(aux.at[other], aux.at[other], aux_send, aux_recv, tp=other).wait_recv()

    def project(base, column, size):
        w = w_in[:, :, :, pl.ds(column, size)].reshape(width, size)
        a = x_all[pl.ds(base, 2)].reshape(2 * rows, width)
        return jnp.dot(a, w, preferred_element_type=F32).astype(BF16)

    def halo_refs(ref, base, tail):
        here = ref.at[pl.ds(base, 2)]
        return here.at[:, pl.ds(rows, tail)], here.at[:, pl.ds(0, tail)]

    def halo_copies(base, turn):
        return ((turn, *halo_refs(kv_rows, base, WINDOW)), (2 + turn, *halo_refs(gated, base, 16)))

    def send_halo(n, src, dst):
        @pl.when(t == 0)
        def _():
            remote(src, dst, halo_send.at[n], halo_recv.at[n], tp=1).start()

        @pl.when(t == 1)
        def _():
            remote(src, dst, halo_send.at[n], halo_recv.at[n], sp=s_next, tp=0).start()

    def wait_halo(n, src, dst):
        remote(dst, dst, halo_send.at[n], halo_recv.at[n], tp=other).wait_recv()

    tiles = 4 * quarter // TILE

    per = quarter // TILE

    def gate(q, carry):
        for n in range(per):
            product = proj[n, q].astype(F32) * proj[(2, 5)[n], q].astype(F32)
            gated[q, 16:, pl.ds(n * TILE, TILE)] = product.astype(BF16)
        return carry

    with jax.named_scope("sinks"):
        aux_lane = lax.broadcasted_iota(jnp.int32, (1, 128), 1)
        heads = quarter // HEAD
        held = aux[f // 2, 8:9, 0:128]
        for h in range(heads):
            one = jnp.sum(jnp.where(aux_lane == first * heads + h, held, 0.0), axis=-1, keepdims=True)
            sink_rows[h : h + 1, :] = jnp.broadcast_to(one * HEAD**0.5, (1, 128))

    at_start = jnp.logical_and(s == 0, t == 0)

    key_id = lax.broadcasted_iota(jnp.int32, (WINDOW, WINDOW), 0)
    query_id = lax.broadcasted_iota(jnp.int32, (WINDOW, WINDOW), 1)
    before = key_id > query_id
    low_keys = lax.broadcasted_iota(jnp.int32, (2 * WINDOW, kvw), 1) < HEAD
    duos = quarter // (2 * HEAD)
    scale = 1.0 / HEAD**0.5

    def attend_block(q, b):
        begin = b * WINDOW
        both = kv_rows[q, begin : begin + 2 * WINDOW, :].astype(F32)
        turned = pltpu.roll(both, HEAD, 1)
        zero = jnp.zeros_like(both)
        keys = jnp.concatenate([jnp.where(low_keys, both, zero), jnp.where(low_keys, zero, turned)], 0).astype(BF16)
        values = jnp.concatenate([jnp.where(low_keys, turned, zero), jnp.where(low_keys, zero, both)], 0)
        values = jnp.transpose(values).astype(BF16)
        scores = []
        for duo in range(duos):
            n, column = 3 + duo * 2 * HEAD // TILE, duo * 2 * HEAD % TILE
            scores.append(rows_dot(keys, proj[n, q, begin : begin + WINDOW, column : column + 2 * HEAD]))
        probs = []
        for duo in range(duos):
            parts = []
            for h in range(2):
                old = scores[duo][2 * h * WINDOW : (2 * h + 1) * WINDOW]
                if b == 0:
                    old = jnp.where(at_start, -jnp.inf, old)
                score = jnp.where(before, old, scores[duo][(2 * h + 1) * WINDOW : (2 * h + 2) * WINDOW])
                sink = sink_rows[2 * duo + h : 2 * duo + h + 1, :]
                peak = jnp.maximum(jnp.max(score, axis=0, keepdims=True), sink)
                weight = jnp.exp((score - peak) * scale)
                total = jnp.sum(weight, axis=0, keepdims=True) + jnp.exp((sink - peak) * scale)
                prob = weight * (1.0 / total)
                parts += [jnp.where(before, prob, 0.0).astype(BF16), jnp.where(before, 0.0, prob).astype(BF16)]
            probs.append(jnp.concatenate(parts, 0))
        for duo in range(duos):
            attended = jnp.dot(values, probs[duo], preferred_element_type=F32)
            span = pl.ds(quarter + duo * 2 * HEAD, 2 * HEAD)
            acts[q, begin : begin + WINDOW, span] = jnp.transpose(attended).astype(BF16)

    def convolve(q, carry):
        for n in range(per):
            span = pl.ds(n * TILE, TILE)
            wide = gated[q, :, span].astype(F32)
            taps = aux[f // 2, 0:TAPS, pl.ds(pl.multiple_of(first * quarter + n * TILE, TILE), TILE)]
            total = (
                pltpu.roll(wide, 2, 0)[16:] * taps[0:1]
                + pltpu.roll(wide, 1, 0)[16:] * taps[1:2]
                + wide[16:] * taps[2:3]
            )
            acts[q, :, span] = (proj[6 + n, q].astype(F32) * total).astype(BF16)
        return carry

    count = width // TILE
    near_half = count // 2
    chips = TILE // (2 * 2 * rb)

    def partial(q, n):
        w = w_out[pl.ds(n * chips, chips)].reshape(TILE, 2 * quarter)
        return rows_dot(acts[q], w)

    ways = (f_next, f_prev)

    def far_copy(way, n):
        return remote(send_far.at[way, n], recv_far.at[way, n], far_send.at[way], far_recv.at[way, n], fs=ways[way])

    def near_copy(way, n):
        return remote(
            send_near.at[way, n], recv_near.at[way, n], near_send.at[way], near_recv.at[way, n], fs=ways[way]
        )

    def far_step(n, carry):
        send_far[0, n] = partial(far_seat, n).astype(BF16)
        send_far[1, n] = partial(far_seat, n + near_half).astype(BF16)
        far_copy(0, n).start()
        far_copy(1, n).start()
        return carry

    def plain_step(n, carry):
        send_near[0, n + near_half] = partial(next_seat, n + near_half).astype(BF16)
        send_near[1, n] = partial(prev_seat, n).astype(BF16)
        near_copy(0, n + near_half).start()
        near_copy(1, n).start()
        return carry

    def joined_step(n, carry):
        right, left = partial(next_seat, n), partial(prev_seat, n + near_half)
        far_copy(0, n).wait_recv()
        far_copy(1, n).wait_recv()
        send_near[0, n] = (right + recv_far[0, n].astype(F32)).astype(BF16)
        send_near[1, n + near_half] = (left + recv_far[1, n].astype(F32)).astype(BF16)
        near_copy(0, n).start()
        near_copy(1, n + near_half).start()
        return carry

    def own_step(n, carry):
        own_sum[n] = partial(mine_seat, n)
        return carry

    def sequences(turn, carry):
        base = lax.rem(f + 1 + turn, 2) * 2
        kv_halo, gated_halo = halo_copies(base, turn)
        count_from = resume + turn * 4 * (last + lag)

        def projection(n, inner):
            ring_half(1, count_from + n)
            pl.when(n == 1)(lambda: send_halo(*kv_halo))
            column = pl.multiple_of(n * TILE + n // 5 * kvw, 128)
            proj[n, pl.ds(base, 2)] = project(base, column, TILE).reshape(2, rows, TILE)
            return inner

        def attend(r, inner):
            for b in range(blocks):
                ring_half(1, count_from + tiles + r * blocks + b)
                attend_block(base + r, b)
                if b == 0:
                    pl.when(r == 0)(lambda: send_halo(*gated_halo))
            return inner

        with jax.named_scope("project_kv"):
            kv_rows[pl.ds(base, 2), WINDOW:, :] = project(base, y_in + quarter, kvw).reshape(2, rows, kvw)
        with jax.named_scope("projections"):
            lax.fori_loop(0, tiles, projection, 0)
        with jax.named_scope("gates"):
            lax.fori_loop(base, base + 2, gate, 0)
        with jax.named_scope("halo_wait"):
            wait_halo(*kv_halo)
        with jax.named_scope("attention"):
            lax.fori_loop(0, 2, attend, 0)
        with jax.named_scope("gated_wait"):
            wait_halo(*gated_halo)

        @pl.when(at_start)
        def _():
            gated[pl.ds(base, 2), 0:16, :] = jnp.zeros((2, 16, quarter), BF16)

        with jax.named_scope("convolution"):
            lax.fori_loop(base, base + 2, convolve, 0)

        @pl.when(turn == 0)
        def _():
            with jax.named_scope("across1"):
                lax.fori_loop(resume + tiles + 2 * blocks, 2 * (last + lag) + 2, lambda u, c: (ring_half(1, u), c)[1], 0)
                wait_across(1)
            with jax.named_scope("plain"):
                lax.fori_loop(0, near_half, plain_step, 0)

        return carry

    lax.fori_loop(0, 2, sequences, 0)
    with jax.named_scope("far"):
        lax.fori_loop(0, near_half, far_step, 0)
    with jax.named_scope("joined"):
        lax.fori_loop(0, near_half, joined_step, 0)
    with jax.named_scope("own"):
        lax.fori_loop(0, count, own_step, 0)
    with jax.named_scope("finish"):
        for n in range(near_half):
            for way, tile in ((0, n + near_half), (1, n)):
                near_copy(way, tile).wait_recv()
        for n in range(near_half):
            for way, tile in ((0, n), (1, n + near_half)):
                near_copy(way, tile).wait_recv()
            for tile in (n, n + near_half):
                total = own_sum[tile] + recv_near[0, tile].astype(F32) + recv_near[1, tile].astype(F32)
                out[:, tile * TILE : (tile + 1) * TILE] = total.astype(BF16)

    for k in range(2):
        for j in range(2):
            here = jnp.logical_and(2 * t + j == f, mine == t)

            @pl.when(jnp.logical_not(here))
            def _():
                piece = weights[k].at[s, t, pl.ds(0, rb), z_span[k]]
                remote(piece, piece, first_send.at[k, j], first_recv.at[k, 0], tp=other).wait_send()

        for way in range(2):
            pieces = weights[k].at[pl.ds(0, ns - 1), 0, pl.ds(0, rb), z_span[k]]
            remote(pieces, pieces, z_send.at[k, way], z_recv.at[k, way, 0, 0], tp=other).wait_send()
        for n, span in ((0, z_span), (1, y_other)):
            piece = weights[k].at[:, t, :, span[k]]
            remote(piece, piece, p_send.at[n, k], p_recv.at[n, k], tp=other).wait_send()
        piece = weights[k].at[:, t, :, y_span[k]]
        remote(piece, piece, y_send.at[k], y_recv.at[k, 0, 0, 0], tp=other).wait_send()
    for way in range(2):
        ref = x_all.at[pl.ds(0, 3), halves[0]]
        remote(ref, ref, x_send.at[way], x_recv.at[way, 0], tp=other).wait_send()
        remote(send_far.at[way], send_far.at[way], far_send.at[way], far_recv.at[way, 0], tp=other).wait_send()
        remote(send_near.at[way], send_near.at[way], near_send.at[way], near_recv.at[way, 0], tp=other).wait_send()
    remote(aux.at[t], aux.at[t], aux_send, aux_recv, tp=other).wait_send()
    for turn in range(2):
        for n, src, dst in halo_copies(2 * turn, turn):
            remote(src, src, halo_send.at[n], halo_recv.at[n], tp=other).wait_send()


def local(
    ns,
    nf,
    tokens,
    norm_gain,
    w_bgate,
    w_cgate,
    w_conv_in,
    conv_taps,
    w_query,
    w_key,
    w_value,
    sink_logits,
    conv_out_weight,
    attn_out_weight,
):
    rows, width = tokens.shape[1:]
    rb, columns = w_query.shape
    quarter = columns // 2
    kvw = w_key.shape[1]
    count = width // TILE
    inside = 4 * quarter + kvw
    vmem = pl.BlockSpec(memory_space=pltpu.VMEM)
    dma = pltpu.SemaphoreType.DMA
    arrays = (
        tokens[0],
        norm_gain[None],
        w_query,
        w_conv_in,
        w_cgate,
        w_bgate,
        w_key,
        w_value,
        conv_taps,
        sink_logits[None],
        conv_out_weight.T,
        attn_out_weight.T,
    )
    out = pl.pallas_call(
        functools.partial(layer_kernel, ns, nf),
        out_shape=jax.ShapeDtypeStruct((rows, width), BF16),
        in_specs=[pl.BlockSpec(memory_space=pltpu.HBM)] * 12,
        out_specs=vmem,
        scratch_shapes=[
            *(pltpu.VMEM(a.shape, a.dtype) for a in arrays),
            pltpu.VMEM((nf, rows, width), BF16),
            pltpu.VMEM((ns, 2, 2 * rb, inside), BF16),
            pltpu.VMEM((ns, 2, 2 * rb, 2 * quarter), BF16),
            pltpu.VMEM((2, rb, kvw), BF16),
            pltpu.VMEM((4 * quarter // TILE, nf, rows, TILE), BF16),
            pltpu.VMEM((nf, WINDOW + rows, kvw), BF16),
            pltpu.VMEM((nf, 16 + rows, quarter), BF16),
            pltpu.VMEM((nf, rows, 2 * quarter), BF16),
            pltpu.VMEM((2, 16, columns), F32),
            pltpu.VMEM((quarter // HEAD, 128), F32),
            pltpu.VMEM((2, count // 2, rows, TILE), BF16),
            pltpu.VMEM((2, count // 2, rows, TILE), BF16),
            pltpu.VMEM((2, count, rows, TILE), BF16),
            pltpu.VMEM((2, count, rows, TILE), BF16),
            pltpu.VMEM((count, rows, TILE), F32),
            dma((2, 2)),
            dma((2, 2)),
            dma((2, 2)),
            dma((2, 2, 2, ns // 2 + 1)),
            dma((2,)),
            dma((2, 2, 2, ns // 2 + 1)),
            dma((2, 2)),
            dma((2, 2)),
            dma((2,)),
            dma((2, 3)),
            dma,
            dma,
            dma((4,)),
            dma((4,)),
            dma((2,)),
            dma((2, count // 2)),
            dma((2,)),
            dma((2, count)),
            dma((len(arrays),)),
        ],
        compiler_params=pltpu.CompilerParams(
            collective_id=0, has_side_effects=True, vmem_limit_bytes=62 * 1024 * 1024
        ),
        name="layer",
    )(*arrays)
    return out[None]


def solution(mesh):
    placed = (
        P(("grp", "fs"), ("sp", "tp"), None),
        P(),
        P(("sp", "fs"), "tp"),
        P(("sp", "fs"), "tp"),
        P(("sp", "fs"), "tp"),
        P(None, "tp"),
        P(("sp", "fs"), "tp"),
        P(("sp", "fs"), "tp"),
        P(("sp", "fs"), "tp"),
        P("tp"),
        P("tp", ("sp", "fs")),
        P("tp", ("sp", "fs")),
    )
    return jax.shard_map(
        functools.partial(local, mesh.shape["sp"], mesh.shape["fs"]),
        mesh=mesh,
        in_specs=placed,
        out_specs=P(("grp", "fs"), ("sp", "tp"), None),
        check_vma=False,
    )
```

```python
import functools

import jax
import jax.numpy as jnp
from jax import lax
from jax.experimental import pallas as pl
from jax.experimental.pallas import tpu as pltpu
from jax.sharding import PartitionSpec as P

HEAD = 64
WINDOW = 128
TAPS = 3
EPSILON = 1e-06
MESH = pl.DeviceIdType.MESH
F32 = jnp.float32
BF16 = jnp.bfloat16
TILE = 256


def rows_dot(a, b):
    return lax.dot_general(a, b, (((1,), (1,)), ((), ())), preferred_element_type=F32)


def layer_kernel(
    ns,
    nf,
    *refs,
):
    given, out, held, rest = refs[:12], refs[12], refs[13:25], refs[25:]
    tokens, gain, w_query, w_conv_in, w_cgate, w_bgate, w_key, w_value, conv_taps, sinks, conv_out, attn_out = held
    (
        x_all,
        w_in,
        w_out,
        kv_pack,
        proj,
        kv_rows,
        gated,
        acts,
        aux,
        sink_rows,
        send_far,
        recv_far,
        send_near,
        recv_near,
        own_sum,
        first_send,
        first_recv,
        z_send,
        z_recv,
        y_send,
        y_recv,
        p_send,
        p_recv,
        out_recv,
        x_send,
        x_recv,
        aux_send,
        aux_recv,
        halo_send,
        halo_recv,
        far_send,
        far_recv,
        near_send,
        near_recv,
        load_sem,
    ) = rest
    g = lax.axis_index("grp")
    s = lax.axis_index("sp")
    f = lax.axis_index("fs")
    t = lax.axis_index("tp")
    odd = lax.rem(g, 2)
    pair = g + 1 - 2 * odd
    s_next, s_prev = lax.rem(s + 1, ns), lax.rem(s + ns - 1, ns)
    f_next, f_prev = lax.rem(f + 1, nf), lax.rem(f + nf - 1, nf)
    f_far = lax.rem(f + 2, nf)
    other = 1 - t

    def seat(q):
        return lax.rem(q, 2) * 2 + q // 2

    mine_seat, far_seat, next_seat, prev_seat = seat(f), seat(f_far), seat(f_next), seat(f_prev)
    rows, width = tokens.shape
    rb = w_query.shape[0]
    quarter = w_query.shape[1] // 2
    kvw = w_key.shape[1]
    half = rows // 2
    blocks = rows // WINDOW

    def remote(src, dst, send_sem, recv_sem, **where):
        return pltpu.make_async_remote_copy(
            src_ref=src,
            dst_ref=dst,
            send_sem=send_sem,
            recv_sem=recv_sem,
            device_id=where,
            device_id_type=MESH,
        )

    loads = [pltpu.make_async_copy(a, b, load_sem.at[n]) for n, (a, b) in enumerate(zip(given, held))]
    for n in (*range(1, len(loads)), 0):
        loads[n].start()

    def when(condition, body):
        if isinstance(condition, bool):
            if condition:
                body()
        else:
            pl.when(condition)(body)

    barrier = pltpu.get_barrier_semaphore()
    greeted = [
        {"fs": lax.rem(f + df, nf), "tp": lax.rem(t + dt, 2)}
        for df in range(nf)
        for dt in range(2)
        if df or dt
    ]
    greeted += [{"sp": z, "tp": lax.rem(t + dt, 2)} for z in (s_next, s_prev) for dt in range(2)]
    greeted.append({"grp": pair})
    for device in greeted:
        pl.semaphore_signal(barrier, inc=1, device_id=device, device_id_type=MESH)

    with jax.named_scope("pack"):
        for load in loads[1:]:
            load.wait()
        low = lax.broadcasted_iota(jnp.int32, (rb, kvw), 1) < HEAD
        keys_wide, values_wide = w_key[...].astype(F32), w_value[...].astype(F32)
        kv_pack[0] = jnp.where(low, keys_wide, pltpu.roll(values_wide, HEAD, 1)).astype(BF16)
        kv_pack[1] = jnp.where(low, pltpu.roll(keys_wide, HEAD, 1), values_wide).astype(BF16)
        aux[t, 0:TAPS, :] = conv_taps[...].astype(F32)
        aux[t, 8:9, 0 : sinks.shape[1]] = sinks[...]
    with jax.named_scope("meet"):
        pl.semaphore_wait(barrier, len(greeted))

    y_in, y_out = quarter + kvw, 3 * quarter // 4
    z_in, z_out = 3 * quarter, 2 * quarter - y_out
    weights = (w_in, w_out)
    lane = pl.multiple_of
    z_span = (pl.ds(lane(odd * y_in, 128), z_in), pl.ds(lane(odd * y_out, 128), z_out))
    y_span = (pl.ds(lane(odd * z_in, 128), y_in), pl.ds(lane(odd * z_out, 128), y_out))
    y_other = (pl.ds(lane((1 - odd) * z_in, 128), y_in), pl.ds(lane((1 - odd) * z_out, 128), y_out))

    mine = f // 2
    first = lax.rem(f, 2)
    slot_rows = pl.ds(pl.multiple_of(first * rb, rb), rb)
    def first_exchange(k):
        for j in range(2):
            to_f = 2 * t + j
            here = jnp.logical_and(to_f == f, mine == t)
            base = j * quarter
            if k == 0:
                at = y_in + quarter
                common = [(w_conv_in, base, y_in, quarter), (w_cgate, base, at, z_in - at)]
                shares = (
                    [(w_query, base, 0, quarter), (kv_pack, None, quarter, kvw)],
                    [(w_cgate, base + z_in - at, z_in, at + quarter - z_in), (w_bgate, base, at + quarter, quarter)],
                )
            else:
                common = []
                shares = (
                    [(conv_out, base, 0, quarter), (attn_out, base, quarter, z_out - quarter)],
                    [(conv_out, base + y_out, y_out, quarter - y_out), (attn_out, base, quarter, quarter)],
                )

            def deliver(moves, here=here, to_f=to_f, j=j, k=k):
                def ends(move):
                    ref, start, column, size = move
                    src = ref.at[j] if start is None else ref.at[:, pl.ds(start, size)]
                    return src, weights[k].at[s, mine, slot_rows, pl.ds(column, size)]

                @pl.when(jnp.logical_not(here))
                def _():
                    for move in moves:
                        src, dst = ends(move)
                        remote(src, dst, first_send.at[k, j], first_recv.at[k, first], fs=to_f, tp=mine).start()

                @pl.when(here)
                def _():
                    for move in moves:
                        src, dst = ends(move)
                        dst[...] = src[...]

            if common:
                deliver(common)
            for parity in range(2):
                pl.when(odd == parity)(functools.partial(deliver, shares[parity]))

    first_exchange(0)
    with jax.named_scope("norm"):
        loads[0].wait()
        step_rows = 32

        def norm(r, carry):
            span = pl.ds(pl.multiple_of(r * step_rows, step_rows), step_rows)
            wide = tokens[span, :].astype(F32)
            scale = lax.rsqrt(jnp.mean(wide * wide, axis=-1, keepdims=True) + EPSILON)
            x_all[mine_seat, span, :] = (wide * scale * gain[...]).astype(BF16)
            return carry

        lax.fori_loop(0, rows // step_rows, norm, 0)
    remote(aux.at[t], aux.at[t], aux_send, aux_recv, tp=other).start()

    def wait_first(k):
        for i in range(2):
            local = jnp.logical_and(t == f // 2, f == 2 * t + i)

            @pl.when(jnp.logical_not(local))
            def _():
                piece = weights[k].at[s, t, pl.ds(i * rb, rb), z_span[k]]
                remote(piece, piece, first_send.at[k, 0], first_recv.at[k, i], tp=other).wait_recv()

    reach = ((ns // 2, ns // 2 - 1), (ns // 2 - 1, ns // 2))

    def onward(k, slot, i, way, hop):
        piece = weights[k].at[slot, t, pl.ds(i * rb, rb), z_span[k]]
        return remote(
            piece, piece, z_send.at[k, way], z_recv.at[k, way, i, hop], sp=(s_next, s_prev)[way]
        )

    def hand_over(k, n, hop, piece):
        recv = (p_recv.at[n], out_recv.at[n, hop])[k]
        return remote(piece, piece, p_send.at[n, k], recv, tp=other)

    def across(k, slot, i, hop):
        hand_over(k, 0, hop, weights[k].at[slot, t, pl.ds(i * rb, rb), z_span[k]]).start()

    def to_pair(k, slot, i, way, hop):
        piece = weights[k].at[slot, t, pl.ds(i * rb, rb), y_span[k]]
        return remote(piece, piece, y_send.at[k], y_recv.at[k, way, i, hop], grp=pair)

    def from_pair(k, slot, i, way, hop):
        piece = weights[k].at[slot, t, pl.ds(i * rb, rb), y_other[k]]
        remote(piece, piece, y_send.at[k], y_recv.at[k, way, i, hop], grp=pair).wait_recv()
        hand_over(k, 1, hop, piece).start()

    def launch(k):
        for i in range(2):
            for way in range(2):
                if reach[way][i] >= 1:
                    onward(k, s, i, way, 1).start()
            to_pair(k, s, i, 0, 0).start()
        for i in range(2):
            across(k, s, i, 0)

    def slot_of(way, hop):
        return lax.rem(s + ns - hop, ns) if way == 0 else lax.rem(s + hop, ns)

    def ring_part(k, hop, i):
        for way in range(2):

            def body(slot=slot_of(way, hop), way=way):
                onward(k, slot, i, way, hop).wait_recv()
                when(hop < reach[way][i], lambda: onward(k, slot, i, way, hop + 1).start())
                to_pair(k, slot, i, way, hop).start()
                across(k, slot, i, hop)

            when(hop <= reach[way][i], body)

    def pair_part(k, hop, i):
        for way in range(2):
            body = functools.partial(from_pair, k, slot_of(way, hop), i, way, hop)
            if isinstance(hop, int):
                when(way <= hop <= reach[way][i], body)
            else:
                when(jnp.logical_and(hop >= way, hop <= reach[way][i]), body)

    def ring_step(k, hop):
        for i in range(2):
            ring_part(k, hop, i)

    def pair_step(k, hop):
        for i in range(2):
            pair_part(k, hop, i)

    lag, out_lag = 2, 1

    def ring_half(k, u):
        hop = u // 2
        for i in range(2):

            @pl.when(lax.rem(u, 2) == i)
            def _():
                pl.when(jnp.logical_and(hop >= 1, hop <= last))(lambda: ring_part(k, hop, i))
                pl.when(jnp.logical_and(hop >= out_lag, hop <= last + out_lag))(lambda: pair_part(k, hop - out_lag, i))

    last = ns // 2

    def wait_across():
        for n, span in ((0, z_span), (1, y_other)):
            hand_over(0, n, 0, w_in.at[:, other, :, span[0]]).wait_recv()

    def ready(hop):
        chips_there = 1 if hop in (0, last) else 2
        for n, span in ((0, z_span), (1, y_other)):
            hand_over(1, n, hop, w_out.at[pl.ds(0, chips_there), other, :, span[1]]).wait_recv()

    with jax.named_scope("first_wait"):
        wait_first(0)
    launch(0)
    first_exchange(1)
    halves = (pl.ds(0, half), pl.ds(half, half))
    for which in (0, 1):
        for way, part, to in ((0, which, f_next), (1, 1 - which, f_prev)):
            ref = x_all.at[mine_seat, halves[part]]
            remote(ref, ref, x_send.at[way], x_recv.at[way, part], fs=to).start()
    early = max(1, ns // 4)
    start_out = max(last - 5, 1)
    ahead = min(1, start_out)
    resume = 2 * (last - start_out + ahead + 1)

    def both_rings(hop):
        ring_step(0, hop)
        if hop >= lag:
            pair_step(0, hop - lag)
        if hop == start_out:
            wait_first(1)
            launch(1)
        second_ring(hop - start_out)

    def second_ring(hop):
        if hop >= 1:
            ring_step(1, hop)
            pair_step(1, hop - out_lag)

    with jax.named_scope("ring0_early"):
        for hop in range(1, early):
            both_rings(hop)

    def x_block(which, part, way, kind):
        ref = x_all.at[which, halves[part]]
        return remote(ref, ref, x_send.at[way], x_recv.at[way, kind], fs=(f_next, f_prev)[way])

    with jax.named_scope("rows_onward"):
        x_block(prev_seat, 0, 0, 0).wait_recv()
        x_block(prev_seat, 0, 0, 2).start()
        x_block(next_seat, 1, 1, 1).wait_recv()
        x_block(next_seat, 1, 1, 2).start()
    with jax.named_scope("ring0_late"):
        for hop in range(early, last + 1):
            both_rings(hop)
    with jax.named_scope("pair_late"):
        for hop in range(max(last + 1 - lag, 0), last + 1):
            pair_step(0, hop)
            if last - hop < ahead:
                second_ring(last - start_out + ahead - (last - hop))
    with jax.named_scope("rows_wait"):
        x_block(prev_seat, 1, 0, 1).wait_recv()
        x_block(next_seat, 0, 1, 0).wait_recv()
        x_block(far_seat, 0, 0, 2).wait_recv()
        x_block(far_seat, 1, 1, 2).wait_recv()
    with jax.named_scope("across0"):
        wait_across()
    remote(aux.at[other], aux.at[other], aux_send, aux_recv, tp=other).wait_recv()

    def project(base, column, size):
        w = w_in[:, :, :, pl.ds(column, size)].reshape(width, size)
        a = x_all[pl.ds(base, 2)].reshape(2 * rows, width)
        return jnp.dot(a, w, preferred_element_type=F32).astype(BF16)

    def halo_refs(ref, base, tail):
        here = ref.at[pl.ds(base, 2)]
        return here.at[:, pl.ds(rows, tail)], here.at[:, pl.ds(0, tail)]

    def halo_copies(base, turn):
        return ((turn, *halo_refs(kv_rows, base, WINDOW)), (2 + turn, *halo_refs(gated, base, 16)))

    def send_halo(n, src, dst):
        @pl.when(t == 0)
        def _():
            remote(src, dst, halo_send.at[n], halo_recv.at[n], tp=1).start()

        @pl.when(t == 1)
        def _():
            remote(src, dst, halo_send.at[n], halo_recv.at[n], sp=s_next, tp=0).start()

    def wait_halo(n, src, dst):
        remote(dst, dst, halo_send.at[n], halo_recv.at[n], tp=other).wait_recv()

    tiles = 4 * quarter // TILE

    per = quarter // TILE

    def gate(q, carry):
        for n in range(per):
            product = proj[per + n, q].astype(F32) * proj[2 * per + n, q].astype(F32)
            gated[q, 16:, pl.ds(n * TILE, TILE)] = product.astype(BF16)
        return carry

    with jax.named_scope("sinks"):
        aux_lane = lax.broadcasted_iota(jnp.int32, (1, 128), 1)
        heads = quarter // HEAD
        held = aux[f // 2, 8:9, 0:128]
        for h in range(heads):
            one = jnp.sum(jnp.where(aux_lane == first * heads + h, held, 0.0), axis=-1, keepdims=True)
            sink_rows[h : h + 1, :] = jnp.broadcast_to(one * HEAD**0.5, (1, 128))

    at_start = jnp.logical_and(s == 0, t == 0)

    key_id = lax.broadcasted_iota(jnp.int32, (WINDOW, WINDOW), 0)
    query_id = lax.broadcasted_iota(jnp.int32, (WINDOW, WINDOW), 1)
    before = key_id > query_id
    low_keys = lax.broadcasted_iota(jnp.int32, (2 * WINDOW, kvw), 1) < HEAD
    duos = quarter // (2 * HEAD)
    scale = 1.0 / HEAD**0.5

    def attend_block(q, b):
        begin = b * WINDOW
        both = kv_rows[q, begin : begin + 2 * WINDOW, :].astype(F32)
        turned = pltpu.roll(both, HEAD, 1)
        zero = jnp.zeros_like(both)
        keys = jnp.concatenate([jnp.where(low_keys, both, zero), jnp.where(low_keys, zero, turned)], 0).astype(BF16)
        values = jnp.concatenate([jnp.where(low_keys, turned, zero), jnp.where(low_keys, zero, both)], 0)
        values = jnp.transpose(values).astype(BF16)
        scores = []
        for duo in range(duos):
            n, column = duo * 2 * HEAD // TILE, duo * 2 * HEAD % TILE
            scores.append(rows_dot(keys, proj[n, q, begin : begin + WINDOW, column : column + 2 * HEAD]))
        probs = []
        for duo in range(duos):
            parts = []
            for h in range(2):
                old = scores[duo][2 * h * WINDOW : (2 * h + 1) * WINDOW]
                if b == 0:
                    old = jnp.where(at_start, -jnp.inf, old)
                score = jnp.where(before, old, scores[duo][(2 * h + 1) * WINDOW : (2 * h + 2) * WINDOW])
                sink = sink_rows[2 * duo + h : 2 * duo + h + 1, :]
                peak = jnp.maximum(jnp.max(score, axis=0, keepdims=True), sink)
                weight = jnp.exp((score - peak) * scale)
                total = jnp.sum(weight, axis=0, keepdims=True) + jnp.exp((sink - peak) * scale)
                prob = weight * (1.0 / total)
                parts += [jnp.where(before, prob, 0.0).astype(BF16), jnp.where(before, 0.0, prob).astype(BF16)]
            probs.append(jnp.concatenate(parts, 0))
        for duo in range(duos):
            attended = jnp.dot(values, probs[duo], preferred_element_type=F32)
            span = pl.ds(quarter + duo * 2 * HEAD, 2 * HEAD)
            acts[q, begin : begin + WINDOW, span] = jnp.transpose(attended).astype(BF16)

    def convolve(q, carry):
        for n in range(per):
            span = pl.ds(n * TILE, TILE)
            wide = gated[q, :, span].astype(F32)
            taps = aux[f // 2, 0:TAPS, pl.ds(pl.multiple_of(first * quarter + n * TILE, TILE), TILE)]
            total = (
                pltpu.roll(wide, 2, 0)[16:] * taps[0:1]
                + pltpu.roll(wide, 1, 0)[16:] * taps[1:2]
                + wide[16:] * taps[2:3]
            )
            acts[q, :, span] = (proj[3 * per + n, q].astype(F32) * total).astype(BF16)
        return carry

    count = width // TILE
    near_half = count // 2
    chips = TILE // (2 * 2 * rb)

    def place(k):
        away = (k + 1) // 2 * (2 * lax.rem(k, 2) - 1) * (2 * lax.rem(s, 2) - 1)
        return lax.rem(s // chips + away + count, count)

    def partial(q, k):
        w = w_out[pl.ds(place(k) * chips, chips)].reshape(TILE, 2 * quarter)
        return rows_dot(acts[q], w)

    ways = (f_next, f_prev)

    def far_copy(way, n):
        return remote(send_far.at[way, n], recv_far.at[way, n], far_send.at[way], far_recv.at[way, n], fs=ways[way])

    def near_copy(way, n):
        return remote(
            send_near.at[way, n], recv_near.at[way, n], near_send.at[way], near_recv.at[way, n], fs=ways[way]
        )

    def far_step(n, carry):
        parts = [partial(far_seat, 2 * n + way).astype(BF16) for way in range(2)]
        for way in range(2):
            send_far[way, n] = parts[way]
        for way in range(2):
            far_copy(way, n).start()
        return carry

    def plain_step(n, carry):
        parts = [partial(q, 2 * n + 1 - way).astype(BF16) for way, q in ((0, next_seat), (1, prev_seat))]
        for way in range(2):
            send_near[way, 2 * n + 1 - way] = parts[way]
        for way in range(2):
            near_copy(way, 2 * n + 1 - way).start()
        return carry

    def joined_step(n, carry):
        parts = [partial(q, 2 * n + way) for way, q in ((0, next_seat), (1, prev_seat))]
        for way in range(2):
            far_copy(way, n).wait_recv()
        for way in range(2):
            send_near[way, 2 * n + way] = (parts[way] + recv_far[way, n].astype(F32)).astype(BF16)
        for way in range(2):
            near_copy(way, 2 * n + way).start()
        return carry

    def own_step(k, carry):
        own_sum[k] = partial(mine_seat, k)
        return carry

    def sequences(turn, carry):
        base = lax.rem(f + 1 + turn, 2) * 2
        kv_halo, gated_halo = halo_copies(base, turn)

        def projection(n, inner):
            pl.when(jnp.logical_and(turn == 0, lax.rem(n, 2) == 0))(lambda: ring_half(1, resume + n // 2))
            pl.when(n == 1)(lambda: send_halo(*kv_halo))
            column = pl.multiple_of(n * TILE + (n + tiles - per) // tiles * kvw, 128)
            proj[n, pl.ds(base, 2)] = project(base, column, TILE).reshape(2, rows, TILE)
            return inner

        def attend(r, inner):
            for b in range(blocks):
                if b == 0:
                    pl.when(turn == 0)(lambda: ring_half(1, resume + tiles // 2 + r))
                attend_block(base + r, b)
                if b == 0:
                    pl.when(r == 0)(lambda: send_halo(*gated_halo))
            return inner

        with jax.named_scope("project_kv"):
            kv_rows[pl.ds(base, 2), WINDOW:, :] = project(base, quarter, kvw).reshape(2, rows, kvw)
        with jax.named_scope("projections"):
            lax.fori_loop(0, tiles, projection, 0)
        with jax.named_scope("gates"):
            lax.fori_loop(base, base + 2, gate, 0)
        with jax.named_scope("halo_wait"):
            wait_halo(*kv_halo)
        with jax.named_scope("attention"):
            lax.fori_loop(0, 2, attend, 0)
        with jax.named_scope("gated_wait"):
            wait_halo(*gated_halo)

        @pl.when(at_start)
        def _():
            gated[pl.ds(base, 2), 0:16, :] = jnp.zeros((2, 16, quarter), BF16)

        with jax.named_scope("convolution"):
            lax.fori_loop(base, base + 2, convolve, 0)

        @pl.when(turn == 0)
        def _():
            with jax.named_scope("across1"):
                rest = resume + tiles // 2 + 2
                lax.fori_loop(rest, max(rest, 2 * (last + out_lag) + 2), lambda u, c: (ring_half(1, u), c)[1], 0)
                for hop in range(last + 1):
                    ready(hop)
            with jax.named_scope("plain"):
                lax.fori_loop(0, near_half, plain_step, 0)

        return carry

    lax.fori_loop(0, 2, sequences, 0)
    with jax.named_scope("far"):
        lax.fori_loop(0, near_half, far_step, 0)
    with jax.named_scope("joined"):
        lax.fori_loop(0, near_half, joined_step, 0)
    with jax.named_scope("own"):
        lax.fori_loop(0, count, own_step, 0)
    with jax.named_scope("finish"):
        for n in range(near_half):
            for way in range(2):
                near_copy(way, 2 * n + 1 - way).wait_recv()
        for n in range(near_half):
            for way in range(2):
                near_copy(way, 2 * n + way).wait_recv()
            for k in (2 * n, 2 * n + 1):
                total = own_sum[k] + recv_near[0, k].astype(F32) + recv_near[1, k].astype(F32)
                out[:, pl.ds(pl.multiple_of(place(k) * TILE, TILE), TILE)] = total.astype(BF16)

    for k in range(2):
        for j in range(2):
            here = jnp.logical_and(2 * t + j == f, mine == t)

            @pl.when(jnp.logical_not(here))
            def _():
                piece = weights[k].at[s, t, pl.ds(0, rb), z_span[k]]
                remote(piece, piece, first_send.at[k, j], first_recv.at[k, 0], tp=other).wait_send()

        for way in range(2):
            pieces = weights[k].at[pl.ds(0, ns - 1), 0, pl.ds(0, rb), z_span[k]]
            remote(pieces, pieces, z_send.at[k, way], z_recv.at[k, way, 0, 0], tp=other).wait_send()
        for n, span in ((0, z_span), (1, y_other)):
            piece = weights[k].at[:, t, :, span[k]]
            hand_over(k, n, 0, piece).wait_send()
        piece = weights[k].at[:, t, :, y_span[k]]
        remote(piece, piece, y_send.at[k], y_recv.at[k, 0, 0, 0], tp=other).wait_send()
    for way in range(2):
        ref = x_all.at[pl.ds(0, 3), halves[0]]
        remote(ref, ref, x_send.at[way], x_recv.at[way, 0], tp=other).wait_send()
        remote(send_far.at[way], send_far.at[way], far_send.at[way], far_recv.at[way, 0], tp=other).wait_send()
        remote(send_near.at[way], send_near.at[way], near_send.at[way], near_recv.at[way, 0], tp=other).wait_send()
    remote(aux.at[t], aux.at[t], aux_send, aux_recv, tp=other).wait_send()
    for turn in range(2):
        for n, src, dst in halo_copies(2 * turn, turn):
            remote(src, src, halo_send.at[n], halo_recv.at[n], tp=other).wait_send()


def local(
    ns,
    nf,
    tokens,
    norm_gain,
    w_bgate,
    w_cgate,
    w_conv_in,
    conv_taps,
    w_query,
    w_key,
    w_value,
    sink_logits,
    conv_out_weight,
    attn_out_weight,
):
    rows, width = tokens.shape[1:]
    rb, columns = w_query.shape
    quarter = columns // 2
    kvw = w_key.shape[1]
    count = width // TILE
    inside = 4 * quarter + kvw
    vmem = pl.BlockSpec(memory_space=pltpu.VMEM)
    dma = pltpu.SemaphoreType.DMA
    arrays = (
        tokens[0],
        norm_gain[None],
        w_query,
        w_conv_in,
        w_cgate,
        w_bgate,
        w_key,
        w_value,
        conv_taps,
        sink_logits[None],
        conv_out_weight.T,
        attn_out_weight.T,
    )
    out = pl.pallas_call(
        functools.partial(layer_kernel, ns, nf),
        out_shape=jax.ShapeDtypeStruct((rows, width), BF16),
        in_specs=[pl.BlockSpec(memory_space=pltpu.HBM)] * 12,
        out_specs=vmem,
        scratch_shapes=[
            *(pltpu.VMEM(a.shape, a.dtype) for a in arrays),
            pltpu.VMEM((nf, rows, width), BF16),
            pltpu.VMEM((ns, 2, 2 * rb, inside), BF16),
            pltpu.VMEM((ns, 2, 2 * rb, 2 * quarter), BF16),
            pltpu.VMEM((2, rb, kvw), BF16),
            pltpu.VMEM((4 * quarter // TILE, nf, rows, TILE), BF16),
            pltpu.VMEM((nf, WINDOW + rows, kvw), BF16),
            pltpu.VMEM((nf, 16 + rows, quarter), BF16),
            pltpu.VMEM((nf, rows, 2 * quarter), BF16),
            pltpu.VMEM((2, 16, columns), F32),
            pltpu.VMEM((quarter // HEAD, 128), F32),
            pltpu.VMEM((2, count // 2, rows, TILE), BF16),
            pltpu.VMEM((2, count // 2, rows, TILE), BF16),
            pltpu.VMEM((2, count, rows, TILE), BF16),
            pltpu.VMEM((2, count, rows, TILE), BF16),
            pltpu.VMEM((count, rows, TILE), F32),
            dma((2, 2)),
            dma((2, 2)),
            dma((2, 2)),
            dma((2, 2, 2, ns // 2 + 1)),
            dma((2,)),
            dma((2, 2, 2, ns // 2 + 1)),
            dma((2, 2)),
            dma((2,)),
            dma((2, ns // 2 + 1)),
            dma((2,)),
            dma((2, 3)),
            dma,
            dma,
            dma((4,)),
            dma((4,)),
            dma((2,)),
            dma((2, count // 2)),
            dma((2,)),
            dma((2, count)),
            dma((len(arrays),)),
        ],
        compiler_params=pltpu.CompilerParams(
            collective_id=0, has_side_effects=True, vmem_limit_bytes=50 * 1024 * 1024
        ),
        name="layer",
    )(*(pltpu.with_memory_space_constraint(a, pltpu.HBM) for a in arrays))
    return out[None]


def solution(mesh):
    placed = (
        P(("grp", "fs"), ("sp", "tp"), None),
        P(),
        P(("sp", "fs"), "tp"),
        P(("sp", "fs"), "tp"),
        P(("sp", "fs"), "tp"),
        P(None, "tp"),
        P(("sp", "fs"), "tp"),
        P(("sp", "fs"), "tp"),
        P(("sp", "fs"), "tp"),
        P("tp"),
        P("tp", ("sp", "fs")),
        P("tp", ("sp", "fs")),
    )
    return jax.shard_map(
        functools.partial(local, mesh.shape["sp"], mesh.shape["fs"]),
        mesh=mesh,
        in_specs=placed,
        out_specs=P(("grp", "fs"), ("sp", "tp"), None),
        check_vma=False,
    )
```

```python
import functools

import jax
import jax.numpy as jnp
from jax import lax
from jax.experimental import pallas as pl
from jax.experimental.pallas import tpu as pltpu
from jax.sharding import PartitionSpec as P

HEAD = 64
WINDOW = 128
TAPS = 3
EPSILON = 1e-06
MESH = pl.DeviceIdType.MESH
F32 = jnp.float32
BF16 = jnp.bfloat16
TILE = 256


def rows_dot(a, b):
    return lax.dot_general(a, b, (((1,), (1,)), ((), ())), preferred_element_type=F32)


def layer_kernel(
    ns,
    nf,
    *refs,
):
    given, out, held, rest = refs[:12], refs[12], refs[13:25], refs[25:]
    tokens, gain, w_query, w_conv_in, w_cgate, w_bgate, w_key, w_value, conv_taps, sinks, conv_out, attn_out = held
    (
        x_all,
        w_in,
        w_out,
        kv_pack,
        proj,
        kv_rows,
        gated,
        acts,
        aux,
        sink_rows,
        send_far,
        recv_far,
        send_near,
        recv_near,
        own_sum,
        started,
        started_kv,
        first_send,
        first_recv,
        z_send,
        z_recv,
        y_send,
        y_recv,
        p_send,
        p_recv,
        x_send,
        x_recv,
        aux_send,
        aux_recv,
        halo_send,
        halo_recv,
        far_send,
        far_recv,
        near_send,
        near_recv,
        load_sem,
    ) = rest
    g = lax.axis_index("grp")
    s = lax.axis_index("sp")
    f = lax.axis_index("fs")
    t = lax.axis_index("tp")
    odd = lax.rem(g, 2)
    pair = g + 1 - 2 * odd
    s_next, s_prev = lax.rem(s + 1, ns), lax.rem(s + ns - 1, ns)
    f_next, f_prev = lax.rem(f + 1, nf), lax.rem(f + nf - 1, nf)
    f_far = lax.rem(f + 2, nf)
    other = 1 - t

    def seat(q):
        return lax.rem(q, 2) * 2 + q // 2

    mine_seat, far_seat, next_seat, prev_seat = seat(f), seat(f_far), seat(f_next), seat(f_prev)
    rows, width = tokens.shape
    rb = w_query.shape[0]
    quarter = w_query.shape[1] // 2
    kvw = w_key.shape[1]
    half = rows // 2
    blocks = rows // WINDOW

    def remote(src, dst, send_sem, recv_sem, **where):
        return pltpu.make_async_remote_copy(
            src_ref=src,
            dst_ref=dst,
            send_sem=send_sem,
            recv_sem=recv_sem,
            device_id=where,
            device_id_type=MESH,
        )

    loads = [pltpu.make_async_copy(a, b, load_sem.at[n]) for n, (a, b) in enumerate(zip(given, held))]
    for n in (*range(1, len(loads)), 0):
        loads[n].start()

    def when(condition, body):
        if isinstance(condition, bool):
            if condition:
                body()
        else:
            pl.when(condition)(body)

    barrier = pltpu.get_barrier_semaphore()
    greeted = [
        {"fs": lax.rem(f + df, nf), "tp": lax.rem(t + dt, 2)}
        for df in range(nf)
        for dt in range(2)
        if df or dt
    ]
    greeted += [{"sp": z, "tp": lax.rem(t + dt, 2)} for z in (s_next, s_prev) for dt in range(2)]
    greeted.append({"grp": pair})
    for device in greeted:
        pl.semaphore_signal(barrier, inc=1, device_id=device, device_id_type=MESH)

    with jax.named_scope("pack"):
        for load in loads[1:]:
            load.wait()
        low = lax.broadcasted_iota(jnp.int32, (rb, kvw), 1) < HEAD
        keys_wide, values_wide = w_key[...].astype(F32), w_value[...].astype(F32)
        kv_pack[0] = jnp.where(low, keys_wide, pltpu.roll(values_wide, HEAD, 1)).astype(BF16)
        kv_pack[1] = jnp.where(low, pltpu.roll(keys_wide, HEAD, 1), values_wide).astype(BF16)
        aux[t, 0:TAPS, :] = conv_taps[...].astype(F32)
        aux[t, 8:9, 0 : sinks.shape[1]] = sinks[...]
    with jax.named_scope("meet"):
        pl.semaphore_wait(barrier, len(greeted))

    y_in, y_out = quarter + kvw, 3 * quarter // 4
    z_in, z_out = 3 * quarter, 2 * quarter - y_out
    weights = (w_in, w_out)
    lane = pl.multiple_of
    z_span = (pl.ds(lane(odd * y_in, 128), z_in), pl.ds(lane(odd * y_out, 128), z_out))
    y_span = (pl.ds(lane(odd * z_in, 128), y_in), pl.ds(lane(odd * z_out, 128), y_out))
    y_other = (pl.ds(lane((1 - odd) * z_in, 128), y_in), pl.ds(lane((1 - odd) * z_out, 128), y_out))

    mine = f // 2
    first = lax.rem(f, 2)
    slot_rows = pl.ds(pl.multiple_of(first * rb, rb), rb)
    def first_exchange(k):
        for j in range(2):
            to_f = 2 * t + j
            here = jnp.logical_and(to_f == f, mine == t)
            base = j * quarter
            if k == 0:
                at = y_in + quarter
                common = [(w_conv_in, base, y_in, quarter), (w_cgate, base, at, z_in - at)]
                shares = (
                    [(w_query, base, 0, quarter), (kv_pack, None, quarter, kvw)],
                    [(w_cgate, base + z_in - at, z_in, at + quarter - z_in), (w_bgate, base, at + quarter, quarter)],
                )
            else:
                common = []
                shares = (
                    [(conv_out, base, 0, quarter), (attn_out, base, quarter, z_out - quarter)],
                    [(conv_out, base + y_out, y_out, quarter - y_out), (attn_out, base, quarter, quarter)],
                )

            def deliver(moves, here=here, to_f=to_f, j=j, k=k):
                def ends(move):
                    ref, start, column, size = move
                    src = ref.at[j] if start is None else ref.at[:, pl.ds(start, size)]
                    return src, weights[k].at[(0, s)[k], mine, slot_rows, pl.ds(column, size)]

                @pl.when(jnp.logical_not(here))
                def _():
                    for move in moves:
                        src, dst = ends(move)
                        remote(src, dst, first_send.at[k, j], first_recv.at[k, first], fs=to_f, tp=mine).start()

                @pl.when(here)
                def _():
                    for move in moves:
                        src, dst = ends(move)
                        dst[...] = src[...]

            if common:
                deliver(common)
            for parity in range(2):
                pl.when(odd == parity)(functools.partial(deliver, shares[parity]))

    first_exchange(0)
    with jax.named_scope("norm"):
        loads[0].wait()
        step_rows = 32

        chunk = width // ns

        def norm(r, carry):
            span = pl.ds(pl.multiple_of(r * step_rows, step_rows), step_rows)
            wide = tokens[span, :].astype(F32)
            scale = lax.rsqrt(jnp.mean(wide * wide, axis=-1, keepdims=True) + EPSILON)
            for p in range(ns):
                away = p // 2 if p % 2 == 0 else ns - (p + 1) // 2
                block = pl.ds(pl.multiple_of(lax.rem(s + away, ns) * chunk, chunk), chunk)
                part = tokens[span, block].astype(F32) * scale * gain[:, block]
                x_all[mine_seat, span, p * chunk : (p + 1) * chunk] = part.astype(BF16)
            return carry

        lax.fori_loop(0, rows // step_rows, norm, 0)
    remote(aux.at[t], aux.at[t], aux_send, aux_recv, tp=other).start()

    def wait_first(k):
        for i in range(2):
            local = jnp.logical_and(t == f // 2, f == 2 * t + i)

            @pl.when(jnp.logical_not(local))
            def _():
                piece = weights[k].at[(0, s)[k], t, pl.ds(i * rb, rb), z_span[k]]
                remote(piece, piece, first_send.at[k, 0], first_recv.at[k, i], tp=other).wait_recv()

    reach = ((ns // 2, ns // 2 - 1), (ns // 2 - 1, ns // 2))

    def slot_of(way, hop):
        return lax.rem(s + ns - hop, ns) if way == 0 else lax.rem(s + hop, ns)

    def spot(k, way, hop):
        if k == 1:
            return slot_of(way, hop)
        return min(max(2 * hop - 1 + way, 0), ns - 1)

    def piece_of(k, way, hop, i, span):
        return weights[k].at[spot(k, way, hop), t, pl.ds(i * rb, rb), span[k]]

    def onward(k, i, way, hop):
        src = piece_of(k, way, hop - 1, i, z_span)
        dst = src if k == 1 else piece_of(k, way, hop, i, z_span)
        return remote(src, dst, z_send.at[k, way], z_recv.at[k, way, i, hop], sp=(s_next, s_prev)[way])

    def arrival(k, i, way, hop):
        piece = piece_of(k, way, hop, i, z_span)
        return remote(piece, piece, z_send.at[k, way], z_recv.at[k, way, i, hop], sp=(s_next, s_prev)[way])

    def hand_over(k, n, hop, piece):
        return remote(piece, piece, p_send.at[k, n], p_recv.at[k, n, hop], tp=other)

    def across(k, i, way, hop):
        hand_over(k, 0, hop, piece_of(k, way, hop, i, z_span)).start()

    def to_pair(k, i, way, hop):
        piece = piece_of(k, way, hop, i, y_span)
        return remote(piece, piece, y_send.at[k], y_recv.at[k, way, i, hop], grp=pair)

    def from_pair(k, i, way, hop):
        piece = piece_of(k, way, hop, i, y_other)
        remote(piece, piece, y_send.at[k], y_recv.at[k, way, i, hop], grp=pair).wait_recv()
        hand_over(k, 1, hop, piece).start()

    def launch(k):
        for i in range(2):
            for way in range(2):
                if reach[way][i] >= 1:
                    onward(k, i, way, 1).start()
            to_pair(k, i, 0, 0).start()
        for i in range(2):
            across(k, i, 0, 0)

    def ring_part(k, hop, i):
        for way in range(2):

            def body(way=way):
                arrival(k, i, way, hop).wait_recv()
                when(hop < reach[way][i], lambda: onward(k, i, way, hop + 1).start())
                to_pair(k, i, way, hop).start()
                across(k, i, way, hop)

            when(hop <= reach[way][i], body)

    def pair_part(k, hop, i):
        for way in range(2):
            body = functools.partial(from_pair, k, i, way, hop)
            if isinstance(hop, int):
                when(way <= hop <= reach[way][i], body)
            else:
                when(jnp.logical_and(hop >= way, hop <= reach[way][i]), body)

    def ring_step(k, hop):
        for i in range(2):
            ring_part(k, hop, i)

    def pair_step(k, hop):
        for i in range(2):
            pair_part(k, hop, i)

    lag, out_lag = 2, 1

    def ring_half(k, u):
        hop = u // 2
        for i in range(2):

            @pl.when(lax.rem(u, 2) == i)
            def _():
                pl.when(jnp.logical_and(hop >= 1, hop <= last))(lambda: ring_part(k, hop, i))
                pl.when(jnp.logical_and(hop >= out_lag, hop <= last + out_lag))(lambda: pair_part(k, hop - out_lag, i))

    last = ns // 2

    def ready(k, hop):
        chips_there = 1 if hop in (0, last) else 2
        for n, span in ((0, z_span), (1, y_other)):
            hand_over(k, n, hop, weights[k].at[pl.ds(0, chips_there), other, :, span[k]]).wait_recv()

    with jax.named_scope("first_wait"):
        wait_first(0)
    launch(0)
    first_exchange(1)
    halves = (pl.ds(0, half), pl.ds(half, half))
    for which in (0, 1):
        for way, part, to in ((0, which, f_next), (1, 1 - which, f_prev)):
            ref = x_all.at[mine_seat, halves[part]]
            remote(ref, ref, x_send.at[way], x_recv.at[way, part], fs=to).start()
    early = max(1, ns // 4)
    soon = max(last - 4, 0)
    soon_blocks = min(2 * soon + 1, ns - 1)
    tiles = 4 * quarter // TILE
    near_base = lax.rem(f + 1, 2) * 2

    def column_of(n):
        return pl.multiple_of(n * TILE + (n + tiles - tiles // 4) // tiles * kvw, 128)

    def product(base, column, size, lo, hi):
        w = w_in[lo:hi, :, :, pl.ds(column, size)].reshape((hi - lo) * chunk, size)
        a = x_all[pl.ds(base, 2), :, lo * chunk : hi * chunk].reshape(2 * rows, (hi - lo) * chunk)
        return jnp.dot(a, w, preferred_element_type=F32)

    def begin_tile(base, n):
        started[n] = product(base, column_of(n), TILE, 0, soon_blocks)

    def begin_kv(base):
        started_kv[...] = product(base, quarter, kvw, 0, soon_blocks)

    def begin(which):
        per_site = tiles // 2 - 1
        lo, hi = which * per_site, min((which + 1) * per_site, tiles)
        with jax.named_scope("begin"):
            lax.fori_loop(lo, hi, lambda n, c: (begin_tile(near_base, n), c)[1], 0)
            if hi == tiles:
                begin_kv(near_base)
    start_out = max(last - 6, 1)
    ahead = min(1, start_out)
    resume = 2 * (last - start_out + ahead + 1)

    def both_rings(hop, whole=True):
        if whole:
            ring_step(0, hop)
        if hop >= lag:
            pair_step(0, hop - lag)
        if hop == start_out:
            wait_first(1)
            launch(1)
        second_ring(hop - start_out)

    def second_ring(hop):
        if hop >= 1:
            ring_step(1, hop)
            pair_step(1, hop - out_lag)

    with jax.named_scope("ring0_early"):
        for hop in range(1, early):
            both_rings(hop)

    def x_block(which, part, way, kind):
        ref = x_all.at[which, halves[part]]
        return remote(ref, ref, x_send.at[way], x_recv.at[way, kind], fs=(f_next, f_prev)[way])

    with jax.named_scope("rows_onward"):
        x_block(prev_seat, 0, 0, 0).wait_recv()
        x_block(prev_seat, 0, 0, 2).start()
        x_block(next_seat, 1, 1, 1).wait_recv()
        x_block(next_seat, 1, 1, 2).start()
    with jax.named_scope("ring0_late"):
        for hop in range(early, last - 1):
            both_rings(hop)
        for hop in range(soon + 1):
            ready(0, hop)
        x_block(prev_seat, 1, 0, 1).wait_recv()
        x_block(next_seat, 0, 1, 0).wait_recv()
        ring_step(0, last - 1)
        begin(0)
        both_rings(last - 1, False)
        begin(1)
        ring_step(0, last)
        begin(2)
        both_rings(last, False)
    with jax.named_scope("pair_late"):
        for hop in range(max(last + 1 - lag, 0), last + 1):
            pair_step(0, hop)
            if last - hop < ahead:
                second_ring(last - start_out + ahead - (last - hop))
    with jax.named_scope("rows_wait"):
        x_block(far_seat, 0, 0, 2).wait_recv()
        x_block(far_seat, 1, 1, 2).wait_recv()
    with jax.named_scope("across0"):
        for hop in range(soon + 1, last + 1):
            ready(0, hop)
    remote(aux.at[other], aux.at[other], aux_send, aux_recv, tp=other).wait_recv()

    def halo_refs(ref, base, tail):
        here = ref.at[pl.ds(base, 2)]
        return here.at[:, pl.ds(rows, tail)], here.at[:, pl.ds(0, tail)]

    def halo_copies(base, turn):
        return ((turn, *halo_refs(kv_rows, base, WINDOW)), (2 + turn, *halo_refs(gated, base, 16)))

    def send_halo(n, src, dst):
        @pl.when(t == 0)
        def _():
            remote(src, dst, halo_send.at[n], halo_recv.at[n], tp=1).start()

        @pl.when(t == 1)
        def _():
            remote(src, dst, halo_send.at[n], halo_recv.at[n], sp=s_next, tp=0).start()

    def wait_halo(n, src, dst):
        remote(dst, dst, halo_send.at[n], halo_recv.at[n], tp=other).wait_recv()

    per = quarter // TILE

    def gate(q, carry):
        for n in range(per):
            product = proj[per + n, q].astype(F32) * proj[2 * per + n, q].astype(F32)
            gated[q, 16:, pl.ds(n * TILE, TILE)] = product.astype(BF16)
        return carry

    with jax.named_scope("sinks"):
        aux_lane = lax.broadcasted_iota(jnp.int32, (1, 128), 1)
        heads = quarter // HEAD
        held = aux[f // 2, 8:9, 0:128]
        for h in range(heads):
            one = jnp.sum(jnp.where(aux_lane == first * heads + h, held, 0.0), axis=-1, keepdims=True)
            sink_rows[h : h + 1, :] = jnp.broadcast_to(one * HEAD**0.5, (1, 128))

    at_start = jnp.logical_and(s == 0, t == 0)

    key_id = lax.broadcasted_iota(jnp.int32, (WINDOW, WINDOW), 0)
    query_id = lax.broadcasted_iota(jnp.int32, (WINDOW, WINDOW), 1)
    before = key_id > query_id
    low_keys = lax.broadcasted_iota(jnp.int32, (2 * WINDOW, kvw), 1) < HEAD
    duos = quarter // (2 * HEAD)
    scale = 1.0 / HEAD**0.5

    def attend_block(q, b):
        begin = b * WINDOW
        both = kv_rows[q, begin : begin + 2 * WINDOW, :].astype(F32)
        turned = pltpu.roll(both, HEAD, 1)
        zero = jnp.zeros_like(both)
        keys = jnp.concatenate([jnp.where(low_keys, both, zero), jnp.where(low_keys, zero, turned)], 0).astype(BF16)
        values = jnp.concatenate([jnp.where(low_keys, turned, zero), jnp.where(low_keys, zero, both)], 0)
        values = jnp.transpose(values).astype(BF16)
        scores = []
        for duo in range(duos):
            n, column = duo * 2 * HEAD // TILE, duo * 2 * HEAD % TILE
            scores.append(rows_dot(keys, proj[n, q, begin : begin + WINDOW, column : column + 2 * HEAD]))
        probs = []
        for duo in range(duos):
            parts = []
            for h in range(2):
                old = scores[duo][2 * h * WINDOW : (2 * h + 1) * WINDOW]
                if b == 0:
                    old = jnp.where(at_start, -jnp.inf, old)
                score = jnp.where(before, old, scores[duo][(2 * h + 1) * WINDOW : (2 * h + 2) * WINDOW])
                sink = sink_rows[2 * duo + h : 2 * duo + h + 1, :]
                peak = jnp.maximum(jnp.max(score, axis=0, keepdims=True), sink)
                weight = jnp.exp((score - peak) * scale)
                total = jnp.sum(weight, axis=0, keepdims=True) + jnp.exp((sink - peak) * scale)
                prob = weight * (1.0 / total)
                parts += [jnp.where(before, prob, 0.0).astype(BF16), jnp.where(before, 0.0, prob).astype(BF16)]
            probs.append(jnp.concatenate(parts, 0))
        for duo in range(duos):
            attended = jnp.dot(values, probs[duo], preferred_element_type=F32)
            span = pl.ds(quarter + duo * 2 * HEAD, 2 * HEAD)
            acts[q, begin : begin + WINDOW, span] = jnp.transpose(attended).astype(BF16)

    def convolve(q, carry):
        for n in range(per):
            span = pl.ds(n * TILE, TILE)
            wide = gated[q, :, span].astype(F32)
            taps = aux[f // 2, 0:TAPS, pl.ds(pl.multiple_of(first * quarter + n * TILE, TILE), TILE)]
            total = (
                pltpu.roll(wide, 2, 0)[16:] * taps[0:1]
                + pltpu.roll(wide, 1, 0)[16:] * taps[1:2]
                + wide[16:] * taps[2:3]
            )
            acts[q, :, span] = (proj[3 * per + n, q].astype(F32) * total).astype(BF16)
        return carry

    count = width // TILE
    near_half = count // 2
    chips = TILE // (2 * 2 * rb)

    def place(k):
        away = (k + 1) // 2 * (2 * lax.rem(k, 2) - 1) * (2 * lax.rem(s, 2) - 1)
        return lax.rem(s // chips + away + count, count)

    def partial(q, k):
        w = w_out[pl.ds(place(k) * chips, chips)].reshape(TILE, 2 * quarter)
        return rows_dot(acts[q], w)

    ways = (f_next, f_prev)

    def far_copy(way, n):
        return remote(send_far.at[way, n], recv_far.at[way, n], far_send.at[way], far_recv.at[way, n], fs=ways[way])

    def near_copy(way, n):
        return remote(
            send_near.at[way, n], recv_near.at[way, n], near_send.at[way], near_recv.at[way, n], fs=ways[way]
        )

    def far_step(n, carry):
        parts = [partial(far_seat, 2 * n + way).astype(BF16) for way in range(2)]
        for way in range(2):
            send_far[way, n] = parts[way]
        for way in range(2):
            far_copy(way, n).start()
        return carry

    def plain_step(n, carry):
        parts = [partial(q, 2 * n + 1 - way).astype(BF16) for way, q in ((0, next_seat), (1, prev_seat))]
        for way in range(2):
            send_near[way, 2 * n + 1 - way] = parts[way]
        for way in range(2):
            near_copy(way, 2 * n + 1 - way).start()
        return carry

    def joined_step(n, carry):
        parts = [partial(q, 2 * n + way) for way, q in ((0, next_seat), (1, prev_seat))]
        for way in range(2):
            far_copy(way, n).wait_recv()
        for way in range(2):
            send_near[way, 2 * n + way] = (parts[way] + recv_far[way, n].astype(F32)).astype(BF16)
        for way in range(2):
            near_copy(way, 2 * n + way).start()
        return carry

    def own_step(k, carry):
        own_sum[k] = partial(mine_seat, k)
        return carry

    def sequences(turn, carry):
        base = lax.rem(f + 1 + turn, 2) * 2
        kv_halo, gated_halo = halo_copies(base, turn)

        def projection(n, inner):
            pl.when(jnp.logical_and(jnp.logical_and(turn == 0, n >= 2), lax.rem(n, 2) == 0))(
                lambda: ring_half(1, resume + n // 2 - 1)
            )
            pl.when(n == 1)(lambda: send_halo(*kv_halo))
            m = lax.rem(n + per, 3 * per) + n // (3 * per) * (2 * per)

            @pl.when(turn == 0)
            def _():
                done = started[m] + product(base, column_of(m), TILE, soon_blocks, ns)
                proj[m, pl.ds(base, 2)] = done.astype(BF16).reshape(2, rows, TILE)

            @pl.when(turn == 1)
            def _():
                done = product(base, column_of(m), TILE, 0, ns)
                proj[m, pl.ds(base, 2)] = done.astype(BF16).reshape(2, rows, TILE)

            @pl.when(n == 2 * per - 1)
            def _():
                lax.fori_loop(base, base + 2, gate, 0)

            pl.when(n == 2 * per + 1)(lambda: send_halo(*gated_halo))
            return inner

        def attend(r, inner):
            for b in range(blocks):
                if b == 0:
                    pl.when(jnp.logical_and(turn == 0, r == 0))(lambda: ring_half(1, resume + tiles // 2 - 1))
                attend_block(base + r, b)
            return inner

        with jax.named_scope("project_kv"):
            pl.when(turn == 1)(lambda: begin_kv(base))
            done = started_kv[...] + product(base, quarter, kvw, soon_blocks, ns)
            kv_rows[pl.ds(base, 2), WINDOW:, :] = done.astype(BF16).reshape(2, rows, kvw)
        with jax.named_scope("projections"):
            lax.fori_loop(0, tiles, projection, 0)
        with jax.named_scope("halo_wait"):
            wait_halo(*kv_halo)
        with jax.named_scope("attention"):
            lax.fori_loop(0, 2, attend, 0)
        with jax.named_scope("gated_wait"):
            wait_halo(*gated_halo)

        @pl.when(at_start)
        def _():
            gated[pl.ds(base, 2), 0:16, :] = jnp.zeros((2, 16, quarter), BF16)

        with jax.named_scope("convolution"):
            lax.fori_loop(base, base + 2, convolve, 0)

        @pl.when(turn == 0)
        def _():
            with jax.named_scope("across1"):
                rest = resume + tiles // 2
                lax.fori_loop(rest, max(rest, 2 * (last + out_lag) + 2), lambda u, c: (ring_half(1, u), c)[1], 0)
                for hop in range(last + 1):
                    ready(1, hop)
            with jax.named_scope("plain"):
                lax.fori_loop(0, near_half, plain_step, 0)

        return carry

    lax.fori_loop(0, 2, sequences, 0)
    with jax.named_scope("far"):
        lax.fori_loop(0, near_half, far_step, 0)
    with jax.named_scope("joined"):
        lax.fori_loop(0, near_half, joined_step, 0)
    with jax.named_scope("own"):
        lax.fori_loop(0, count, own_step, 0)
    with jax.named_scope("finish"):
        for n in range(near_half):
            for way in range(2):
                near_copy(way, 2 * n + 1 - way).wait_recv()
        for n in range(near_half):
            for way in range(2):
                near_copy(way, 2 * n + way).wait_recv()
            for k in (2 * n, 2 * n + 1):
                total = own_sum[k] + recv_near[0, k].astype(F32) + recv_near[1, k].astype(F32)
                out[:, pl.ds(pl.multiple_of(place(k) * TILE, TILE), TILE)] = total.astype(BF16)

    for k in range(2):
        for j in range(2):
            here = jnp.logical_and(2 * t + j == f, mine == t)

            @pl.when(jnp.logical_not(here))
            def _():
                piece = weights[k].at[s, t, pl.ds(0, rb), z_span[k]]
                remote(piece, piece, first_send.at[k, j], first_recv.at[k, 0], tp=other).wait_send()

        for way in range(2):
            pieces = weights[k].at[pl.ds(0, ns - 1), 0, pl.ds(0, rb), z_span[k]]
            remote(pieces, pieces, z_send.at[k, way], z_recv.at[k, way, 0, 0], tp=other).wait_send()
        for n, span in ((0, z_span), (1, y_other)):
            piece = weights[k].at[:, t, :, span[k]]
            hand_over(k, n, 0, piece).wait_send()
        piece = weights[k].at[:, t, :, y_span[k]]
        remote(piece, piece, y_send.at[k], y_recv.at[k, 0, 0, 0], tp=other).wait_send()
    for way in range(2):
        ref = x_all.at[pl.ds(0, 3), halves[0]]
        remote(ref, ref, x_send.at[way], x_recv.at[way, 0], tp=other).wait_send()
        remote(send_far.at[way], send_far.at[way], far_send.at[way], far_recv.at[way, 0], tp=other).wait_send()
        remote(send_near.at[way], send_near.at[way], near_send.at[way], near_recv.at[way, 0], tp=other).wait_send()
    remote(aux.at[t], aux.at[t], aux_send, aux_recv, tp=other).wait_send()
    for turn in range(2):
        for n, src, dst in halo_copies(2 * turn, turn):
            remote(src, src, halo_send.at[n], halo_recv.at[n], tp=other).wait_send()


def local(
    ns,
    nf,
    tokens,
    norm_gain,
    w_bgate,
    w_cgate,
    w_conv_in,
    conv_taps,
    w_query,
    w_key,
    w_value,
    sink_logits,
    conv_out_weight,
    attn_out_weight,
):
    rows, width = tokens.shape[1:]
    rb, columns = w_query.shape
    quarter = columns // 2
    kvw = w_key.shape[1]
    count = width // TILE
    inside = 4 * quarter + kvw
    vmem = pl.BlockSpec(memory_space=pltpu.VMEM)
    dma = pltpu.SemaphoreType.DMA
    arrays = (
        tokens[0],
        norm_gain[None],
        w_query,
        w_conv_in,
        w_cgate,
        w_bgate,
        w_key,
        w_value,
        conv_taps,
        sink_logits[None],
        conv_out_weight.T,
        attn_out_weight.T,
    )
    out = pl.pallas_call(
        functools.partial(layer_kernel, ns, nf),
        out_shape=jax.ShapeDtypeStruct((rows, width), BF16),
        in_specs=[pl.BlockSpec(memory_space=pltpu.HBM)] * 12,
        out_specs=vmem,
        scratch_shapes=[
            *(pltpu.VMEM(a.shape, a.dtype) for a in arrays),
            pltpu.VMEM((nf, rows, width), BF16),
            pltpu.VMEM((ns, 2, 2 * rb, inside), BF16),
            pltpu.VMEM((ns, 2, 2 * rb, 2 * quarter), BF16),
            pltpu.VMEM((2, rb, kvw), BF16),
            pltpu.VMEM((4 * quarter // TILE, nf, rows, TILE), BF16),
            pltpu.VMEM((nf, WINDOW + rows, kvw), BF16),
            pltpu.VMEM((nf, 16 + rows, quarter), BF16),
            pltpu.VMEM((nf, rows, 2 * quarter), BF16),
            pltpu.VMEM((2, 16, columns), F32),
            pltpu.VMEM((quarter // HEAD, 128), F32),
            pltpu.VMEM((2, count // 2, rows, TILE), BF16),
            pltpu.VMEM((2, count // 2, rows, TILE), BF16),
            pltpu.VMEM((2, count, rows, TILE), BF16),
            pltpu.VMEM((2, count, rows, TILE), BF16),
            pltpu.VMEM((count, rows, TILE), F32),
            pltpu.VMEM((4 * quarter // TILE, 2 * rows, TILE), F32),
            pltpu.VMEM((2 * rows, kvw), F32),
            dma((2, 2)),
            dma((2, 2)),
            dma((2, 2)),
            dma((2, 2, 2, ns // 2 + 1)),
            dma((2,)),
            dma((2, 2, 2, ns // 2 + 1)),
            dma((2, 2)),
            dma((2, 2, ns // 2 + 1)),
            dma((2,)),
            dma((2, 3)),
            dma,
            dma,
            dma((4,)),
            dma((4,)),
            dma((2,)),
            dma((2, count // 2)),
            dma((2,)),
            dma((2, count)),
            dma((len(arrays),)),
        ],
        compiler_params=pltpu.CompilerParams(
            collective_id=0, has_side_effects=True, vmem_limit_bytes=50 * 1024 * 1024
        ),
        name="layer",
    )(*(pltpu.with_memory_space_constraint(a, pltpu.HBM) for a in arrays))
    return out[None]


def solution(mesh):
    placed = (
        P(("grp", "fs"), ("sp", "tp"), None),
        P(),
        P(("sp", "fs"), "tp"),
        P(("sp", "fs"), "tp"),
        P(("sp", "fs"), "tp"),
        P(None, "tp"),
        P(("sp", "fs"), "tp"),
        P(("sp", "fs"), "tp"),
        P(("sp", "fs"), "tp"),
        P("tp"),
        P("tp", ("sp", "fs")),
        P("tp", ("sp", "fs")),
    )
    return jax.shard_map(
        functools.partial(local, mesh.shape["sp"], mesh.shape["fs"]),
        mesh=mesh,
        in_specs=placed,
        out_specs=P(("grp", "fs"), ("sp", "tp"), None),
        check_vma=False,
    )
```

```python
import functools

import jax
import jax.numpy as jnp
from jax import lax
from jax.experimental import pallas as pl
from jax.experimental.pallas import tpu as pltpu
from jax.sharding import PartitionSpec as P

HEAD = 64
WINDOW = 128
TAPS = 3
EPSILON = 1e-06
MESH = pl.DeviceIdType.MESH
F32 = jnp.float32
BF16 = jnp.bfloat16
TILE = 256


def rows_dot(a, b):
    return lax.dot_general(a, b, (((1,), (1,)), ((), ())), preferred_element_type=F32)


def layer_kernel(
    ns,
    nf,
    *refs,
):
    given, out, held, rest = refs[:12], refs[12], refs[13:25], refs[25:]
    tokens, gain, w_query, w_conv_in, w_cgate, w_bgate, w_key, w_value, conv_taps, sinks, conv_out, attn_out = held
    (
        x_all,
        w_in,
        w_out,
        kv_pack,
        proj,
        kv_rows,
        gated,
        acts,
        aux,
        sink_rows,
        send_far,
        recv_far,
        send_near,
        recv_near,
        own_sum,
        started,
        started_kv,
        first_send,
        first_recv,
        z_send,
        z_recv,
        y_send,
        y_recv,
        p_send,
        p_recv,
        x_send,
        x_recv,
        aux_send,
        aux_recv,
        halo_send,
        halo_recv,
        far_send,
        far_recv,
        near_send,
        near_recv,
        load_sem,
    ) = rest
    g = lax.axis_index("grp")
    s = lax.axis_index("sp")
    f = lax.axis_index("fs")
    t = lax.axis_index("tp")
    odd = lax.rem(g, 2)
    pair = g + 1 - 2 * odd
    s_next, s_prev = lax.rem(s + 1, ns), lax.rem(s + ns - 1, ns)
    f_next, f_prev = lax.rem(f + 1, nf), lax.rem(f + nf - 1, nf)
    f_far = lax.rem(f + 2, nf)
    other = 1 - t

    def seat(q):
        return lax.rem(q, 2) * 2 + q // 2

    mine_seat, far_seat, next_seat, prev_seat = seat(f), seat(f_far), seat(f_next), seat(f_prev)
    rows, width = tokens.shape
    rb = w_query.shape[0]
    quarter = w_query.shape[1] // 2
    kvw = w_key.shape[1]
    half = rows // 2
    blocks = rows // WINDOW

    def remote(src, dst, send_sem, recv_sem, **where):
        return pltpu.make_async_remote_copy(
            src_ref=src,
            dst_ref=dst,
            send_sem=send_sem,
            recv_sem=recv_sem,
            device_id=where,
            device_id_type=MESH,
        )

    loads = [pltpu.make_async_copy(a, b, load_sem.at[n]) for n, (a, b) in enumerate(zip(given, held))]
    for n in (*range(1, len(loads)), 0):
        loads[n].start()

    def when(condition, body):
        if isinstance(condition, bool):
            if condition:
                body()
        else:
            pl.when(condition)(body)

    barrier = pltpu.get_barrier_semaphore()
    greeted = [
        {"fs": lax.rem(f + df, nf), "tp": lax.rem(t + dt, 2)}
        for df in range(nf)
        for dt in range(2)
        if df or dt
    ]
    greeted += [{"sp": z, "tp": lax.rem(t + dt, 2)} for z in (s_next, s_prev) for dt in range(2)]
    greeted.append({"grp": pair})
    for device in greeted:
        pl.semaphore_signal(barrier, inc=1, device_id=device, device_id_type=MESH)

    with jax.named_scope("pack"):
        for load in loads[1:]:
            load.wait()
        low = lax.broadcasted_iota(jnp.int32, (rb, kvw), 1) < HEAD
        keys_wide, values_wide = w_key[...].astype(F32), w_value[...].astype(F32)
        kv_pack[0] = jnp.where(low, keys_wide, pltpu.roll(values_wide, HEAD, 1)).astype(BF16)
        kv_pack[1] = jnp.where(low, pltpu.roll(keys_wide, HEAD, 1), values_wide).astype(BF16)
        aux[t, 0:TAPS, :] = conv_taps[...].astype(F32)
        aux[t, 8:9, 0 : sinks.shape[1]] = sinks[...]
    with jax.named_scope("meet"):
        pl.semaphore_wait(barrier, len(greeted))

    y_in, y_out = quarter + kvw, 3 * quarter // 4
    z_in, z_out = 3 * quarter, 2 * quarter - y_out
    weights = (w_in, w_out)
    lane = pl.multiple_of
    z_span = (pl.ds(lane(odd * y_in, 128), z_in), pl.ds(lane(odd * y_out, 128), z_out))
    y_span = (pl.ds(lane(odd * z_in, 128), y_in), pl.ds(lane(odd * z_out, 128), y_out))
    y_other = (pl.ds(lane((1 - odd) * z_in, 128), y_in), pl.ds(lane((1 - odd) * z_out, 128), y_out))

    mine = f // 2
    first = lax.rem(f, 2)
    slot_rows = pl.ds(pl.multiple_of(first * rb, rb), rb)
    def first_exchange(k):
        for j in range(2):
            to_f = 2 * t + j
            here = jnp.logical_and(to_f == f, mine == t)
            base = j * quarter
            if k == 0:
                at = y_in + quarter
                common = [(w_conv_in, base, y_in, quarter), (w_cgate, base, at, z_in - at)]
                shares = (
                    [(w_query, base, 0, quarter), (kv_pack, None, quarter, kvw)],
                    [(w_cgate, base + z_in - at, z_in, at + quarter - z_in), (w_bgate, base, at + quarter, quarter)],
                )
            else:
                common = []
                shares = (
                    [(conv_out, base, 0, quarter), (attn_out, base, quarter, z_out - quarter)],
                    [(conv_out, base + y_out, y_out, quarter - y_out), (attn_out, base, quarter, quarter)],
                )

            def deliver(moves, here=here, to_f=to_f, j=j, k=k):
                def ends(move):
                    ref, start, column, size = move
                    src = ref.at[j] if start is None else ref.at[:, pl.ds(start, size)]
                    return src, weights[k].at[(0, s)[k], mine, slot_rows, pl.ds(column, size)]

                @pl.when(jnp.logical_not(here))
                def _():
                    for move in moves:
                        src, dst = ends(move)
                        remote(src, dst, first_send.at[k, j], first_recv.at[k, first], fs=to_f, tp=mine).start()

                @pl.when(here)
                def _():
                    for move in moves:
                        src, dst = ends(move)
                        dst[...] = src[...]

            if common:
                deliver(common)
            for parity in range(2):
                pl.when(odd == parity)(functools.partial(deliver, shares[parity]))

    first_exchange(0)
    with jax.named_scope("norm"):
        loads[0].wait()
        step_rows = 32

        chunk = width // ns

        def norm(r, carry):
            span = pl.ds(pl.multiple_of(r * step_rows, step_rows), step_rows)
            wide = tokens[span, :].astype(F32)
            scale = lax.rsqrt(jnp.mean(wide * wide, axis=-1, keepdims=True) + EPSILON)
            for p in range(ns):
                away = p // 2 if p % 2 == 0 else ns - (p + 1) // 2
                block = pl.ds(pl.multiple_of(lax.rem(s + away, ns) * chunk, chunk), chunk)
                part = tokens[span, block].astype(F32) * scale * gain[:, block]
                x_all[mine_seat, span, p * chunk : (p + 1) * chunk] = part.astype(BF16)
            return carry

        lax.fori_loop(0, rows // step_rows, norm, 0)
    remote(aux.at[t], aux.at[t], aux_send, aux_recv, tp=other).start()

    def wait_first(k, i):
        local = jnp.logical_and(t == f // 2, f == 2 * t + i)

        @pl.when(jnp.logical_not(local))
        def _():
            piece = weights[k].at[(0, s)[k], t, pl.ds(i * rb, rb), z_span[k]]
            remote(piece, piece, first_send.at[k, 0], first_recv.at[k, i], tp=other).wait_recv()

    reach = ((ns // 2, ns // 2 - 1), (ns // 2 - 1, ns // 2))

    def slot_of(way, hop):
        return lax.rem(s + ns - hop, ns) if way == 0 else lax.rem(s + hop, ns)

    def spot(k, way, hop):
        if k == 1:
            return slot_of(way, hop)
        return min(max(2 * hop - 1 + way, 0), ns - 1)

    def piece_of(k, way, hop, i, span):
        return weights[k].at[spot(k, way, hop), t, pl.ds(i * rb, rb), span[k]]

    def onward(k, i, way, hop):
        src = piece_of(k, way, hop - 1, i, z_span)
        dst = src if k == 1 else piece_of(k, way, hop, i, z_span)
        return remote(src, dst, z_send.at[k, way], z_recv.at[k, way, i, hop], sp=(s_next, s_prev)[way])

    def arrival(k, i, way, hop):
        piece = piece_of(k, way, hop, i, z_span)
        return remote(piece, piece, z_send.at[k, way], z_recv.at[k, way, i, hop], sp=(s_next, s_prev)[way])

    def hand_over(k, n, hop, piece):
        return remote(piece, piece, p_send.at[k, n], p_recv.at[k, n, hop], tp=other)

    def across(k, i, way, hop):
        hand_over(k, 0, hop, piece_of(k, way, hop, i, z_span)).start()

    def to_pair(k, i, way, hop):
        piece = piece_of(k, way, hop, i, y_span)
        return remote(piece, piece, y_send.at[k], y_recv.at[k, way, i, hop], grp=pair)

    def from_pair(k, i, way, hop):
        piece = piece_of(k, way, hop, i, y_other)
        remote(piece, piece, y_send.at[k], y_recv.at[k, way, i, hop], grp=pair).wait_recv()
        hand_over(k, 1, hop, piece).start()

    def launch(k):
        for i in range(2):
            wait_first(k, i)
            for way in range(2):
                if reach[way][i] >= 1:
                    onward(k, i, way, 1).start()
            to_pair(k, i, 0, 0).start()
        for i in range(2):
            across(k, i, 0, 0)

    def ring_part(k, hop, i):
        for way in range(2):

            def body(way=way):
                arrival(k, i, way, hop).wait_recv()
                when(hop < reach[way][i], lambda: onward(k, i, way, hop + 1).start())
                to_pair(k, i, way, hop).start()
                across(k, i, way, hop)

            when(hop <= reach[way][i], body)

    def pair_part(k, hop, i):
        for way in range(2):
            body = functools.partial(from_pair, k, i, way, hop)
            if isinstance(hop, int):
                when(way <= hop <= reach[way][i], body)
            else:
                when(jnp.logical_and(hop >= way, hop <= reach[way][i]), body)

    def ring_step(k, hop):
        for i in range(2):
            ring_part(k, hop, i)

    def pair_step(k, hop):
        for i in range(2):
            pair_part(k, hop, i)

    lag, out_lag = 2, 1

    def ring_half(k, u):
        hop = u // 2
        for i in range(2):

            @pl.when(lax.rem(u, 2) == i)
            def _():
                pl.when(jnp.logical_and(hop >= 1, hop <= last))(lambda: ring_part(k, hop, i))
                pl.when(jnp.logical_and(hop >= out_lag, hop <= last + out_lag))(lambda: pair_part(k, hop - out_lag, i))

    last = ns // 2

    def ready(k, hop):
        chips_there = 1 if hop in (0, last) else 2
        for n, span in ((0, z_span), (1, y_other)):
            hand_over(k, n, hop, weights[k].at[pl.ds(0, chips_there), other, :, span[k]]).wait_recv()

    with jax.named_scope("first_wait"):
        launch(0)
    first_exchange(1)
    halves = (pl.ds(0, half), pl.ds(half, half))
    for which in (0, 1):
        for way, part, to in ((0, which, f_next), (1, 1 - which, f_prev)):
            ref = x_all.at[mine_seat, halves[part]]
            remote(ref, ref, x_send.at[way], x_recv.at[way, part], fs=to).start()
    early = max(1, ns // 4)
    soon = max(last - 4, 0)
    soon_blocks = min(2 * soon + 1, ns - 1)
    tiles = 4 * quarter // TILE
    near_base = lax.rem(f + 1, 2) * 2

    def column_of(n):
        return pl.multiple_of(n * TILE + (n + tiles - tiles // 4) // tiles * kvw, 128)

    def product(base, column, size, lo, hi):
        w = w_in[lo:hi, :, :, pl.ds(column, size)].reshape((hi - lo) * chunk, size)
        a = x_all[pl.ds(base, 2), :, lo * chunk : hi * chunk].reshape(2 * rows, (hi - lo) * chunk)
        return jnp.dot(a, w, preferred_element_type=F32)

    def begin_tile(base, n):
        started[n] = product(base, column_of(n), TILE, 0, soon_blocks)

    def begin_kv(base):
        started_kv[...] = product(base, quarter, kvw, 0, soon_blocks)

    def begin(which):
        per_site = tiles // 2 - 1
        lo, hi = which * per_site, min((which + 1) * per_site, tiles)
        with jax.named_scope("begin"):
            lax.fori_loop(lo, hi, lambda n, c: (begin_tile(near_base, n), c)[1], 0)
            if hi == tiles:
                begin_kv(near_base)
    start_out = max(last - 6, 1)
    ahead = min(1, start_out)
    resume = 2 * (last - start_out + ahead + 1)

    def both_rings(hop, whole=True):
        if whole:
            ring_step(0, hop)
        if hop >= lag:
            pair_step(0, hop - lag)
        if hop == start_out:
            launch(1)
        second_ring(hop - start_out)

    def second_ring(hop):
        if hop >= 1:
            ring_step(1, hop)
            pair_step(1, hop - out_lag)

    with jax.named_scope("ring0_early"):
        for hop in range(1, early):
            both_rings(hop)

    def x_block(which, part, way, kind):
        ref = x_all.at[which, halves[part]]
        return remote(ref, ref, x_send.at[way], x_recv.at[way, kind], fs=(f_next, f_prev)[way])

    with jax.named_scope("rows_onward"):
        x_block(prev_seat, 0, 0, 0).wait_recv()
        x_block(prev_seat, 0, 0, 2).start()
        x_block(next_seat, 1, 1, 1).wait_recv()
        x_block(next_seat, 1, 1, 2).start()
    with jax.named_scope("ring0_late"):
        for hop in range(early, last - 1):
            both_rings(hop)
        for hop in range(soon + 1):
            ready(0, hop)
        x_block(prev_seat, 1, 0, 1).wait_recv()
        x_block(next_seat, 0, 1, 0).wait_recv()
        ring_step(0, last - 1)
        begin(0)
        both_rings(last - 1, False)
        begin(1)
        ring_step(0, last)
        begin(2)
        both_rings(last, False)
    with jax.named_scope("pair_late"):
        for hop in range(max(last + 1 - lag, 0), last + 1):
            pair_step(0, hop)
            if last - hop < ahead:
                second_ring(last - start_out + ahead - (last - hop))
    with jax.named_scope("rows_wait"):
        x_block(far_seat, 0, 0, 2).wait_recv()
        x_block(far_seat, 1, 1, 2).wait_recv()
    with jax.named_scope("across0"):
        for hop in range(soon + 1, last + 1):
            ready(0, hop)
    remote(aux.at[other], aux.at[other], aux_send, aux_recv, tp=other).wait_recv()

    def halo_refs(ref, base, tail):
        here = ref.at[pl.ds(base, 2)]
        return here.at[:, pl.ds(rows, tail)], here.at[:, pl.ds(0, tail)]

    def halo_copies(base, turn):
        return ((turn, *halo_refs(kv_rows, base, WINDOW)), (2 + turn, *halo_refs(gated, base, 16)))

    def send_halo(n, src, dst):
        @pl.when(t == 0)
        def _():
            remote(src, dst, halo_send.at[n], halo_recv.at[n], tp=1).start()

        @pl.when(t == 1)
        def _():
            remote(src, dst, halo_send.at[n], halo_recv.at[n], sp=s_next, tp=0).start()

    def wait_halo(n, src, dst):
        remote(dst, dst, halo_send.at[n], halo_recv.at[n], tp=other).wait_recv()

    per = quarter // TILE

    def gate(q, carry):
        for n in range(per):
            product = proj[per + n, q].astype(F32) * proj[2 * per + n, q].astype(F32)
            gated[q, 16:, pl.ds(n * TILE, TILE)] = product.astype(BF16)
        return carry

    with jax.named_scope("sinks"):
        aux_lane = lax.broadcasted_iota(jnp.int32, (1, 128), 1)
        heads = quarter // HEAD
        held = aux[f // 2, 8:9, 0:128]
        for h in range(heads):
            one = jnp.sum(jnp.where(aux_lane == first * heads + h, held, 0.0), axis=-1, keepdims=True)
            sink_rows[h : h + 1, :] = jnp.broadcast_to(one * HEAD**0.5, (1, 128))

    at_start = jnp.logical_and(s == 0, t == 0)

    key_id = lax.broadcasted_iota(jnp.int32, (WINDOW, WINDOW), 0)
    query_id = lax.broadcasted_iota(jnp.int32, (WINDOW, WINDOW), 1)
    before = key_id > query_id
    low_keys = lax.broadcasted_iota(jnp.int32, (2 * WINDOW, kvw), 1) < HEAD
    duos = quarter // (2 * HEAD)
    scale = 1.0 / HEAD**0.5

    def attend_block(q, b):
        begin = b * WINDOW
        both = kv_rows[q, begin : begin + 2 * WINDOW, :].astype(F32)
        turned = pltpu.roll(both, HEAD, 1)
        zero = jnp.zeros_like(both)
        keys = jnp.concatenate([jnp.where(low_keys, both, zero), jnp.where(low_keys, zero, turned)], 0).astype(BF16)
        values = jnp.concatenate([jnp.where(low_keys, turned, zero), jnp.where(low_keys, zero, both)], 0)
        values = jnp.transpose(values).astype(BF16)
        scores = []
        for duo in range(duos):
            n, column = duo * 2 * HEAD // TILE, duo * 2 * HEAD % TILE
            scores.append(rows_dot(keys, proj[n, q, begin : begin + WINDOW, column : column + 2 * HEAD]))
        probs = []
        for duo in range(duos):
            parts = []
            for h in range(2):
                old = scores[duo][2 * h * WINDOW : (2 * h + 1) * WINDOW]
                if b == 0:
                    old = jnp.where(at_start, -jnp.inf, old)
                score = jnp.where(before, old, scores[duo][(2 * h + 1) * WINDOW : (2 * h + 2) * WINDOW])
                sink = sink_rows[2 * duo + h : 2 * duo + h + 1, :]
                peak = jnp.maximum(jnp.max(score, axis=0, keepdims=True), sink)
                weight = jnp.exp((score - peak) * scale)
                total = jnp.sum(weight, axis=0, keepdims=True) + jnp.exp((sink - peak) * scale)
                prob = weight * (1.0 / total)
                parts += [jnp.where(before, prob, 0.0).astype(BF16), jnp.where(before, 0.0, prob).astype(BF16)]
            probs.append(jnp.concatenate(parts, 0))
        for duo in range(duos):
            attended = jnp.dot(values, probs[duo], preferred_element_type=F32)
            span = pl.ds(quarter + duo * 2 * HEAD, 2 * HEAD)
            acts[q, begin : begin + WINDOW, span] = jnp.transpose(attended).astype(BF16)

    def convolve(q, carry):
        for n in range(per):
            span = pl.ds(n * TILE, TILE)
            wide = gated[q, :, span].astype(F32)
            taps = aux[f // 2, 0:TAPS, pl.ds(pl.multiple_of(first * quarter + n * TILE, TILE), TILE)]
            total = (
                pltpu.roll(wide, 2, 0)[16:] * taps[0:1]
                + pltpu.roll(wide, 1, 0)[16:] * taps[1:2]
                + wide[16:] * taps[2:3]
            )
            acts[q, :, span] = (proj[3 * per + n, q].astype(F32) * total).astype(BF16)
        return carry

    count = width // TILE
    near_half = count // 2
    chips = TILE // (2 * 2 * rb)

    def place(k):
        away = (k + 1) // 2 * (2 * lax.rem(k, 2) - 1) * (2 * lax.rem(s, 2) - 1)
        return lax.rem(s // chips + away + count, count)

    def partial(q, k):
        w = w_out[pl.ds(place(k) * chips, chips)].reshape(TILE, 2 * quarter)
        return rows_dot(acts[q], w)

    ways = (f_next, f_prev)

    def far_copy(way, n):
        return remote(send_far.at[way, n], recv_far.at[way, n], far_send.at[way], far_recv.at[way, n], fs=ways[way])

    def near_copy(way, n):
        return remote(
            send_near.at[way, n], recv_near.at[way, n], near_send.at[way], near_recv.at[way, n], fs=ways[way]
        )

    def far_step(n, carry):
        parts = [partial(far_seat, 2 * n + way).astype(BF16) for way in range(2)]
        for way in range(2):
            send_far[way, n] = parts[way]
        for way in range(2):
            far_copy(way, n).start()
        return carry

    def plain_step(n, carry):
        parts = [partial(q, 2 * n + 1 - way).astype(BF16) for way, q in ((0, next_seat), (1, prev_seat))]
        for way in range(2):
            send_near[way, 2 * n + 1 - way] = parts[way]
        for way in range(2):
            near_copy(way, 2 * n + 1 - way).start()
        return carry

    def joined_step(n, carry):
        parts = [partial(q, 2 * n + way) for way, q in ((0, next_seat), (1, prev_seat))]
        for way in range(2):
            far_copy(way, n).wait_recv()
        for way in range(2):
            send_near[way, 2 * n + way] = (parts[way] + recv_far[way, n].astype(F32)).astype(BF16)
        for way in range(2):
            near_copy(way, 2 * n + way).start()
        return carry

    def own_step(k, carry):
        own_sum[k] = partial(mine_seat, k)
        return carry

    def sequences(turn, carry):
        base = lax.rem(f + 1 + turn, 2) * 2
        kv_halo, gated_halo = halo_copies(base, turn)

        def projection(n, inner):
            pl.when(jnp.logical_and(jnp.logical_and(turn == 0, n >= 2), lax.rem(n, 2) == 0))(
                lambda: ring_half(1, resume + n // 2 - 1)
            )
            pl.when(n == 1)(lambda: send_halo(*kv_halo))
            m = lax.rem(n + per, 3 * per) + n // (3 * per) * (2 * per)

            @pl.when(turn == 0)
            def _():
                done = started[m] + product(base, column_of(m), TILE, soon_blocks, ns)
                proj[m, pl.ds(base, 2)] = done.astype(BF16).reshape(2, rows, TILE)

            @pl.when(turn == 1)
            def _():
                done = product(base, column_of(m), TILE, 0, ns)
                proj[m, pl.ds(base, 2)] = done.astype(BF16).reshape(2, rows, TILE)

            @pl.when(n == 2 * per - 1)
            def _():
                lax.fori_loop(base, base + 2, gate, 0)

            pl.when(n == 2 * per + 1)(lambda: send_halo(*gated_halo))
            return inner

        def attend(r, inner):
            for b in range(blocks):
                if b == 0:
                    pl.when(jnp.logical_and(turn == 0, r == 0))(lambda: ring_half(1, resume + tiles // 2 - 1))
                attend_block(base + r, b)
            return inner

        with jax.named_scope("project_kv"):
            pl.when(turn == 1)(lambda: begin_kv(base))
            done = started_kv[...] + product(base, quarter, kvw, soon_blocks, ns)
            kv_rows[pl.ds(base, 2), WINDOW:, :] = done.astype(BF16).reshape(2, rows, kvw)
        with jax.named_scope("projections"):
            lax.fori_loop(0, tiles, projection, 0)
        with jax.named_scope("halo_wait"):
            wait_halo(*kv_halo)
        with jax.named_scope("attention"):
            lax.fori_loop(0, 2, attend, 0)
        with jax.named_scope("gated_wait"):
            wait_halo(*gated_halo)

        @pl.when(at_start)
        def _():
            gated[pl.ds(base, 2), 0:16, :] = jnp.zeros((2, 16, quarter), BF16)

        with jax.named_scope("convolution"):
            lax.fori_loop(base, base + 2, convolve, 0)

        @pl.when(turn == 0)
        def _():
            with jax.named_scope("across1"):
                rest = resume + tiles // 2
                lax.fori_loop(rest, max(rest, 2 * (last + out_lag) + 2), lambda u, c: (ring_half(1, u), c)[1], 0)
                for hop in range(last + 1):
                    ready(1, hop)
            with jax.named_scope("plain"):
                lax.fori_loop(0, near_half, plain_step, 0)

        return carry

    lax.fori_loop(0, 2, sequences, 0)
    with jax.named_scope("far"):
        lax.fori_loop(0, near_half, far_step, 0)
    with jax.named_scope("joined"):
        lax.fori_loop(0, near_half, joined_step, 0)
    with jax.named_scope("own"):
        lax.fori_loop(0, count, own_step, 0)
    with jax.named_scope("finish"):
        for n in range(near_half):
            for way in range(2):
                near_copy(way, 2 * n + 1 - way).wait_recv()
        for n in range(near_half):
            for way in range(2):
                near_copy(way, 2 * n + way).wait_recv()
            for k in (2 * n, 2 * n + 1):
                total = own_sum[k] + recv_near[0, k].astype(F32) + recv_near[1, k].astype(F32)
                out[:, pl.ds(pl.multiple_of(place(k) * TILE, TILE), TILE)] = total.astype(BF16)

    with jax.named_scope("drain"):
        for k in range(2):
            for j in range(2):
                here = jnp.logical_and(2 * t + j == f, mine == t)

                @pl.when(jnp.logical_not(here))
                def _():
                    piece = weights[k].at[s, t, pl.ds(0, rb), z_span[k]]
                    remote(piece, piece, first_send.at[k, j], first_recv.at[k, 0], tp=other).wait_send()

            for way in range(2):
                pieces = weights[k].at[pl.ds(0, ns - 1), 0, pl.ds(0, rb), z_span[k]]
                remote(pieces, pieces, z_send.at[k, way], z_recv.at[k, way, 0, 0], tp=other).wait_send()
            for n, span in ((0, z_span), (1, y_other)):
                piece = weights[k].at[:, t, :, span[k]]
                hand_over(k, n, 0, piece).wait_send()
            piece = weights[k].at[:, t, :, y_span[k]]
            remote(piece, piece, y_send.at[k], y_recv.at[k, 0, 0, 0], tp=other).wait_send()
        for way in range(2):
            ref = x_all.at[pl.ds(0, 3), halves[0]]
            remote(ref, ref, x_send.at[way], x_recv.at[way, 0], tp=other).wait_send()
            remote(send_far.at[way], send_far.at[way], far_send.at[way], far_recv.at[way, 0], tp=other).wait_send()
            remote(send_near.at[way], send_near.at[way], near_send.at[way], near_recv.at[way, 0], tp=other).wait_send()
        remote(aux.at[t], aux.at[t], aux_send, aux_recv, tp=other).wait_send()
        for turn in range(2):
            for n, src, dst in halo_copies(2 * turn, turn):
                remote(src, src, halo_send.at[n], halo_recv.at[n], tp=other).wait_send()


def local(
    ns,
    nf,
    tokens,
    norm_gain,
    w_bgate,
    w_cgate,
    w_conv_in,
    conv_taps,
    w_query,
    w_key,
    w_value,
    sink_logits,
    conv_out_weight,
    attn_out_weight,
):
    rows, width = tokens.shape[1:]
    rb, columns = w_query.shape
    quarter = columns // 2
    kvw = w_key.shape[1]
    count = width // TILE
    inside = 4 * quarter + kvw
    vmem = pl.BlockSpec(memory_space=pltpu.VMEM)
    dma = pltpu.SemaphoreType.DMA
    arrays = (
        tokens[0],
        norm_gain[None],
        w_query,
        w_conv_in,
        w_cgate,
        w_bgate,
        w_key,
        w_value,
        conv_taps,
        sink_logits[None],
        conv_out_weight.T,
        attn_out_weight.T,
    )
    out = pl.pallas_call(
        functools.partial(layer_kernel, ns, nf),
        out_shape=jax.ShapeDtypeStruct((rows, width), BF16),
        in_specs=[pl.BlockSpec(memory_space=pltpu.HBM)] * 12,
        out_specs=vmem,
        scratch_shapes=[
            *(pltpu.VMEM(a.shape, a.dtype) for a in arrays),
            pltpu.VMEM((nf, rows, width), BF16),
            pltpu.VMEM((ns, 2, 2 * rb, inside), BF16),
            pltpu.VMEM((ns, 2, 2 * rb, 2 * quarter), BF16),
            pltpu.VMEM((2, rb, kvw), BF16),
            pltpu.VMEM((4 * quarter // TILE, nf, rows, TILE), BF16),
            pltpu.VMEM((nf, WINDOW + rows, kvw), BF16),
            pltpu.VMEM((nf, 16 + rows, quarter), BF16),
            pltpu.VMEM((nf, rows, 2 * quarter), BF16),
            pltpu.VMEM((2, 16, columns), F32),
            pltpu.VMEM((quarter // HEAD, 128), F32),
            pltpu.VMEM((2, count // 2, rows, TILE), BF16),
            pltpu.VMEM((2, count // 2, rows, TILE), BF16),
            pltpu.VMEM((2, count, rows, TILE), BF16),
            pltpu.VMEM((2, count, rows, TILE), BF16),
            pltpu.VMEM((count, rows, TILE), F32),
            pltpu.VMEM((4 * quarter // TILE, 2 * rows, TILE), F32),
            pltpu.VMEM((2 * rows, kvw), F32),
            dma((2, 2)),
            dma((2, 2)),
            dma((2, 2)),
            dma((2, 2, 2, ns // 2 + 1)),
            dma((2,)),
            dma((2, 2, 2, ns // 2 + 1)),
            dma((2, 2)),
            dma((2, 2, ns // 2 + 1)),
            dma((2,)),
            dma((2, 3)),
            dma,
            dma,
            dma((4,)),
            dma((4,)),
            dma((2,)),
            dma((2, count // 2)),
            dma((2,)),
            dma((2, count)),
            dma((len(arrays),)),
        ],
        compiler_params=pltpu.CompilerParams(
            collective_id=0, has_side_effects=True, vmem_limit_bytes=50 * 1024 * 1024
        ),
        name="layer",
    )(*(pltpu.with_memory_space_constraint(a, pltpu.HBM) for a in arrays))
    return out[None]


def solution(mesh):
    placed = (
        P(("grp", "fs"), ("sp", "tp"), None),
        P(),
        P(("sp", "fs"), "tp"),
        P(("sp", "fs"), "tp"),
        P(("sp", "fs"), "tp"),
        P(None, "tp"),
        P(("sp", "fs"), "tp"),
        P(("sp", "fs"), "tp"),
        P(("sp", "fs"), "tp"),
        P("tp"),
        P("tp", ("sp", "fs")),
        P("tp", ("sp", "fs")),
    )
    return jax.shard_map(
        functools.partial(local, mesh.shape["sp"], mesh.shape["fs"]),
        mesh=mesh,
        in_specs=placed,
        out_specs=P(("grp", "fs"), ("sp", "tp"), None),
        check_vma=False,
    )
```
